256 devices in a mesh: sp: 64 (over z, x, core), tp: 4 (over y).
Axes of the slice: x: 4, y: 4, z: 8, core: 2. Of those that a mesh axis runs over, the one named last changes fastest.
Arguments:
- stream: bfloat16 [16384, 2048], P(('sp', 'tp')), may hold values from -6 to 6
- query_a: bfloat16 [16384, 384], P('sp', 'tp'), may hold values from -400 to 400
- query_b: bfloat16 [16384, 640], P('sp', 'tp'), may hold values from -400 to 400
- latent: bfloat16 [16384, 256], P('sp'), may hold values from -6 to 6
- rotary_key: bfloat16 [16384, 32], P('sp'), may hold values from -6 to 6
- latent_gain: float32 [256], replicated, may hold values from 0.1 to 1.9
- key_gain_a: float32 [96], replicated, may hold values from 0.1 to 1.9
- key_gain_b: float32 [160], replicated, may hold values from 0.1 to 1.9
- w_key_a: bfloat16 [256, 256], P(None, 'tp'), may hold values from -0.375 to 0.375
- w_value_a: bfloat16 [256, 256], P(None, 'tp'), may hold values from -0.375 to 0.375
- w_key_b: bfloat16 [256, 512], P(None, 'tp'), may hold values from -0.375 to 0.375
- w_value_b: bfloat16 [256, 512], P(None, 'tp'), may hold values from -0.375 to 0.375
- w_out_a: bfloat16 [256, 2048], P('tp'), may hold values from -0.21875 to 0.21875
- w_out_b: bfloat16 [512, 2048], P('tp'), may hold values from -0.21875 to 0.21875
- norm_gain: float32 [2048], replicated, may hold values from 0.1 to 1.9
- w_up: bfloat16 [2048, 4096], P('sp', 'tp'), may hold values from -0.125 to 0.125
- w_down: bfloat16 [4096, 2048], P('tp', 'sp'), may hold values from -0.09375 to 0.09375
Outputs:
- result: bfloat16 [16384, 2048], P(('sp', 'tp'))
The draws below stay inside these ranges and needn't reach their ends.
All inputs are finite; a program needn't handle non-finite values.
Results may differ from the reference program's by a relative error of at most 0.018.
The reference program's roundings to bfloat16 on the way count: a program that leaves them out, or rounds other values in their place, can miss the bound.
Values may be sent and summed in bfloat16 or wider, within the bound.
A program may use at most 128 MiB of HBM per device.

```python
import math
import jax
import jax.numpy as jnp
from jax import lax

D = 2048
HEADS_A = 4
HEADS_B = 4
NOPE_A = 64
V_A = 64
NOPE_B = 128
V_B = 128
ROPE = 32
KV_RANK = 256
FF = 4096
TOKENS = 16384


def scaled_rows(key, count, width):
    base_key = jax.random.fold_in(key, 0)
    base = jax.random.normal(base_key, (count, width), jnp.float32)
    factor = 2.5 * jnp.ones((count, 1), jnp.float32)
    return jnp.clip(base * factor, -400.0, 400.0)


def draw_query_a(key, part):
    return scaled_rows(jax.random.fold_in(key, 11), TOKENS, HEADS_A * (NOPE_A + ROPE)).astype(jnp.bfloat16)


def draw_query_b(key, part):
    return scaled_rows(jax.random.fold_in(key, 23), TOKENS, HEADS_B * (NOPE_B + ROPE)).astype(jnp.bfloat16)


def block_scale(stream_key, shape, shards, smallest, largest):
    level = 1.0
    for position, blocks in shards:
        heights = jax.random.uniform(jax.random.fold_in(jax.random.fold_in(stream_key, 6), position), (blocks,), jnp.float32, smallest / len(shards), largest / len(shards))
        level = level * jnp.repeat(jnp.exp(heights), shape[position] // blocks).reshape((-1,) + (1,) * (len(shape) - 1 - position))
    return level


def scatter_about(own_key, shape, scale, reach, cuts=(), kind=jnp.bfloat16):
    array = scale * jax.random.normal(own_key, shape, jnp.float32)
    if cuts:
        array = array * block_scale(own_key, shape, cuts, -0.22, 0.18)
    return jnp.clip(array, -reach, reach).astype(kind)


def setup_inputs(seed: int = 0) -> dict:
    splits = jax.random.split(jax.random.key(seed), 18)
    stream = scatter_about(splits[0], (TOKENS, D), 0.4, 6.0, ((0, 256),))
    query_a = draw_query_a(jax.random.fold_in(splits[17], 71), 0)
    query_b = draw_query_b(jax.random.fold_in(splits[17], 71), 0)
    latent = scatter_about(splits[3], (TOKENS, KV_RANK), 1.0, 6.0, ((0, 64),))
    rotary_key = scatter_about(splits[4], (TOKENS, ROPE), 1.0, 6.0, ((0, 64),))
    latent_gain = jnp.clip(1.0 + 0.18 * jax.random.normal(splits[5], (KV_RANK,), jnp.float32), 0.1, 1.9)
    key_gain_a = jnp.clip(1.0 + 0.18 * jax.random.normal(splits[6], (NOPE_A + ROPE,), jnp.float32), 0.1, 1.9)
    key_gain_b = jnp.clip(1.0 + 0.18 * jax.random.normal(splits[7], (NOPE_B + ROPE,), jnp.float32), 0.1, 1.9)
    w_key_a = scatter_about(splits[8], (KV_RANK, HEADS_A * NOPE_A), KV_RANK ** -0.5, 0.375, ((1, 4),))
    w_value_a = scatter_about(splits[9], (KV_RANK, HEADS_A * V_A), KV_RANK ** -0.5, 0.375, ((1, 4),))
    w_key_b = scatter_about(splits[10], (KV_RANK, HEADS_B * NOPE_B), KV_RANK ** -0.5, 0.375, ((1, 4),))
    w_value_b = scatter_about(splits[11], (KV_RANK, HEADS_B * V_B), KV_RANK ** -0.5, 0.375, ((1, 4),))
    w_out_a = scatter_about(splits[12], (HEADS_A * V_A, D), (HEADS_A * V_A + HEADS_B * V_B) ** -0.5, 0.21875, ((0, 4),))
    w_out_b = scatter_about(splits[13], (HEADS_B * V_B, D), (HEADS_A * V_A + HEADS_B * V_B) ** -0.5, 0.21875, ((0, 4),))
    norm_gain = jnp.clip(1.0 + 0.18 * jax.random.normal(splits[14], (D,), jnp.float32), 0.1, 1.9)
    w_up = scatter_about(splits[15], (D, FF), D ** -0.5, 0.125, ((0, 64), (1, 4)))
    w_down = scatter_about(splits[16], (FF, D), FF ** -0.5, 0.09375, ((0, 4), (1, 64)))
    return {"stream": stream, "query_a": query_a, "query_b": query_b, "latent": latent, "rotary_key": rotary_key, "latent_gain": latent_gain, "key_gain_a": key_gain_a, "key_gain_b": key_gain_b, "w_key_a": w_key_a, "w_value_a": w_value_a, "w_key_b": w_key_b, "w_value_b": w_value_b, "w_out_a": w_out_a, "w_out_b": w_out_b, "norm_gain": norm_gain, "w_up": w_up, "w_down": w_down}


EPSILON = 1e-06
THETA = 10000.0

def rms_scale(values, gain):
    wide = values.astype(jnp.float32)
    return wide * lax.rsqrt(lax.optimization_barrier(jnp.mean(wide * wide, axis=-1, keepdims=True)) + EPSILON) * gain.astype(jnp.float32)

def rotate(tail, positions):
    half = tail.shape[-1] // 2
    freqs = THETA ** (-jnp.arange(half, dtype=jnp.float32) / half)
    angle = positions[:, None, None] * freqs
    cosine = jnp.cos(angle)
    sine = jnp.sin(angle)
    first = tail[..., :half]
    second = tail[..., half:]
    return jnp.concatenate([first * cosine - second * sine, second * cosine + first * sine], axis=-1)

def make_keys(normed, rotary_key, w_key, w_value, key_gain, nope, positions):
    count = normed.shape[0]
    heads = w_key.shape[1] // nope
    head_nope = jnp.dot(normed, w_key, preferred_element_type=jnp.float32).astype(jnp.bfloat16)
    head_nope = head_nope.reshape(count, heads, nope)
    values = jnp.dot(normed, w_value, preferred_element_type=jnp.float32).astype(jnp.bfloat16)
    shared = jnp.broadcast_to(rotary_key[:, None, :], (count, heads, rotary_key.shape[1]))
    joined = rms_scale(jnp.concatenate([head_nope, shared], axis=-1), key_gain)
    turned = rotate(joined[..., nope:], positions)
    keys_out = jnp.concatenate([joined[..., :nope], turned], axis=-1).astype(jnp.bfloat16)
    return (keys_out.reshape(count, -1), values)

def attention(queries, keys_in, values_in, depth):
    total_rows = keys_in.shape[0]
    heads = keys_in.shape[1] // depth
    key_view = keys_in.astype(jnp.float32).reshape(total_rows, heads, depth)
    value_view = values_in.astype(jnp.float32).reshape(total_rows, heads, -1)
    block = math.gcd(queries.shape[0], 512)
    blocks = queries.astype(jnp.float32).reshape(-1, block, heads, depth)

    def one_block(block_queries):
        scores = jnp.einsum('qhd,khd->qhk', block_queries, key_view) * depth ** (-0.5)
        peak = lax.optimization_barrier(jnp.max(scores, axis=-1))
        shifted = jnp.exp(scores - peak[..., None])
        totals = lax.optimization_barrier(jnp.sum(shifted, axis=-1))
        weights = lax.optimization_barrier(shifted.astype(jnp.bfloat16)).astype(jnp.float32)
        weighted = jnp.einsum('qhk,khd->qhd', weights, value_view)
        return (weighted / totals[..., None]).astype(jnp.bfloat16).reshape(block, -1)
    return lax.map(one_block, blocks).reshape(queries.shape[0], -1)

def reference(stream, query_a, query_b, latent, rotary_key, latent_gain, key_gain_a, key_gain_b, w_key_a, w_value_a, w_key_b, w_value_b, w_out_a, w_out_b, norm_gain, w_up, w_down):
    positions = jnp.arange(TOKENS).astype(jnp.float32)
    normed_latent = rms_scale(latent, latent_gain).astype(jnp.bfloat16)
    key_a, value_a = make_keys(normed_latent, rotary_key, w_key_a, w_value_a, key_gain_a, NOPE_A, positions)
    key_b, value_b = make_keys(normed_latent, rotary_key, w_key_b, w_value_b, key_gain_b, NOPE_B, positions)
    attended_a = attention(query_a, key_a, value_a, NOPE_A + ROPE)
    attended_b = attention(query_b, key_b, value_b, NOPE_B + ROPE)
    mixed = jnp.dot(attended_a, w_out_a, preferred_element_type=jnp.float32) + jnp.dot(attended_b, w_out_b, preferred_element_type=jnp.float32)
    residual = (stream.astype(jnp.float32) + mixed).astype(jnp.bfloat16)
    normed = rms_scale(residual, norm_gain).astype(jnp.bfloat16)
    activated = jnp.square(jax.nn.relu(jnp.dot(normed, w_up, preferred_element_type=jnp.float32))).astype(jnp.bfloat16)
    summed = jnp.dot(activated, w_down, preferred_element_type=jnp.float32)
    return (residual.astype(jnp.float32) + summed).astype(jnp.bfloat16)
```

```python
import functools
import math

import jax
import jax.numpy as jnp
from jax import lax
from jax.experimental import pallas as pl
from jax.experimental.pallas import tpu as pltpu
from jax.sharding import PartitionSpec as P

NOPE_A = 64
V_A = 64
NOPE_B = 128
V_B = 128
ROPE = 32
DEPTH_A = NOPE_A + ROPE
DEPTH_B = NOPE_B + ROPE
KV = NOPE_A + NOPE_B + V_A + V_B
OUT = V_A + V_B
RANK = 256
D = 2048
FF = 1024
TOK = 256
OWN = 64
Z, X, C, Y = 8, 4, 2, 4
EPSILON = 1e-06
THETA = 10000.0
LOG2E = 1.4426950408889634
SCALE_A = DEPTH_A ** (-0.5) * LOG2E
SCALE_B = DEPTH_B ** (-0.5) * LOG2E
NT = (((1,), (1,)), ((), ()))
NN = (((1,), (0,)), ((), ()))
F32 = jnp.float32
BF16 = jnp.bfloat16


def mm(a, b, dims):
    return lax.dot_general(a, b, dims, preferred_element_type=F32)


def kernel(
    lat_in,
    q_in,
    up_in,
    dn_in,
    woa_in,
    wob_in,
    st_in,
    wt,
    lgain,
    kgain,
    ngain,
    trig,
    out,
    lat,
    qb,
    up,
    dn,
    wo,
    st,
    kta,
    ktb,
    ka,
    kb,
    va,
    vb,
    oacc,
    stat,
    osend,
    orecv,
    srecv,
    att,
    res,
    nrm,
    act,
    pb,
    rb,
    loc,
    lat_s,
    lat_r,
    latp_s,
    latp_r,
    q_s,
    q_r,
    upx_s,
    upx_r,
    upz_s,
    upz_r,
    upp_s,
    upp_r,
    dnz_s,
    dnz_r,
    dnx_s,
    dnx_r,
    dnp_s,
    dnp_r,
    st_s,
    st_r,
    wo_s,
    wo_r,
    wop_s,
    wop_r,
    ox_s,
    ox_r,
    sx_s,
    sx_r,
    ay_s,
    ay_r,
    rs_s,
    rs_r,
):
    sp = lax.axis_index("sp")
    y = lax.axis_index("tp")
    z = lax.div(sp, 8)
    x = lax.rem(lax.div(sp, 2), 4)
    c = lax.rem(sp, 2)
    oc = 1 - c

    def wrap(v, n):
        return lax.rem(v + 2 * n, n)

    def dev(z_, x_, c_, y_):
        return {"sp": z_ * 8 + x_ * 2 + c_, "tp": y_}

    partner = dev(z, x, oc, y)
    zdev = (dev(wrap(z + 1, Z), x, c, y), dev(wrap(z - 1, Z), x, c, y))
    xdev = [None] + [dev(z, wrap(x + d, X), c, y) for d in (1, 2, 3)]
    ydev = [None] + [dev(z, x, c, wrap(y + d, Y)) for d in (1, 2, 3)]

    def rdma(src, dst, ss, rs, where):
        return pltpu.make_async_remote_copy(
            src_ref=src,
            dst_ref=dst,
            send_sem=ss,
            recv_sem=rs,
            device_id=where,
            device_id_type=pl.DeviceIdType.MESH,
        )

    def same(ref, ss, rs, where):
        return rdma(ref, ref, ss, rs, where)

    locals_ = [
        pltpu.make_async_copy(lat_in, lat.at[z, c], loc.at[0]),
        pltpu.make_async_copy(q_in, qb.at[x], loc.at[1]),
        pltpu.make_async_copy(up_in, up.at[z, x, c], loc.at[2]),
        pltpu.make_async_copy(dn_in, dn.at[z, x, c], loc.at[3]),
        pltpu.make_async_copy(st_in, st.at[y], loc.at[4]),
        pltpu.make_async_copy(woa_in, wo.at[y, pl.ds(0, V_A)], loc.at[5]),
        pltpu.make_async_copy(wob_in, wo.at[y, pl.ds(V_A, V_B)], loc.at[6]),
    ]
    for cp in locals_:
        cp.start()

    barrier = pltpu.get_barrier_semaphore()
    for where in [partner, *zdev, *xdev[1:], *ydev[1:]]:
        pl.semaphore_signal(
            barrier, inc=1, device_id=where, device_id_type=pl.DeviceIdType.MESH
        )

    kta[...] = jnp.zeros_like(kta)
    ktb[...] = jnp.zeros_like(ktb)
    oacc[...] = jnp.zeros_like(oacc)
    for j in range(X):
        stat[j] = jnp.zeros((8, TOK), F32)
        stat[j, 0:1] = jnp.full((1, TOK), -jnp.inf, F32)
        stat[j, 2:3] = jnp.full((1, TOK), -jnp.inf, F32)

    def lat_ring(way, s, zsrc):
        return same(lat.at[zsrc, c], lat_s.at[way, s], lat_r.at[way, s], zdev[way])

    def lat_part(way, s, zsrc):
        return same(lat.at[zsrc, c], latp_s.at[way, s], latp_r.at[way, s], partner)

    def q_x(d):
        return same(qb.at[x], q_s.at[d - 1], q_r.at[d - 1], xdev[d])

    def up_x(d):
        return same(up.at[z, x, c], upx_s.at[d - 1], upx_r.at[d - 1], xdev[d])

    def up_ring(way, s, zsrc):
        return same(up.at[zsrc, :, c], upz_s.at[way, s], upz_r.at[way, s], zdev[way])

    def up_part(way, s, zsrc):
        return same(up.at[zsrc, :, c], upp_s.at[way, s], upp_r.at[way, s], partner)

    def dn_ring(way, s, zsrc):
        return same(dn.at[zsrc, x, c], dnz_s.at[way, s], dnz_r.at[way, s], zdev[way])

    def dn_x(d, zsrc):
        return same(dn.at[zsrc, x, c], dnx_s.at[d - 1], dnx_r.at[d - 1], xdev[d])

    def dn_x_all(d):
        return same(dn.at[:, wrap(x - d, X), c], dnx_s.at[d - 1], dnx_r.at[d - 1], xdev[d])

    def dn_part(d):
        return same(dn.at[:, wrap(x - d, X), c], dnp_s.at[d], dnp_r.at[d], partner)

    def st_y(d):
        return same(st.at[y], st_s.at[d - 1], st_r.at[d - 1], ydev[d])

    half = pl.ds(pl.multiple_of(c * (D // 2), D // 2), D // 2)

    def wo_y(d):
        return same(wo.at[y, :, half], wo_s.at[d - 1], wo_r.at[d - 1], ydev[d])

    def wo_part(d):
        return same(
            wo.at[wrap(y - d, Y), :, half], wop_s.at[d - 1], wop_r.at[d - 1], partner
        )

    def o_x(d):
        return rdma(
            osend.at[wrap(x + d, X)], orecv.at[x], ox_s.at[d - 1], ox_r.at[d - 1], xdev[d]
        )

    def s_x(d):
        return rdma(
            stat.at[wrap(x + d, X)], srecv.at[x], sx_s.at[d - 1], sx_r.at[d - 1], xdev[d]
        )

    def a_y(d):
        return same(att.at[y], ay_s.at[d - 1], ay_r.at[d - 1], ydev[d])

    def r_y(d, n):
        return rdma(
            pb.at[n, wrap(y + d, Y)],
            rb.at[y, n],
            rs_s.at[d - 1, n],
            rs_r.at[d - 1, n],
            ydev[d],
        )

    for cp in locals_:
        cp.wait()
    pl.semaphore_wait(barrier, 9)

    lat_ring(0, 1, z).start()
    lat_ring(1, 1, z).start()
    lat_part(0, 0, z).start()
    for d in (2, 1, 3):
        q_x(d).start()
    for way in (0, 1):
        dn_ring(way, 1, z).start()
    for d in (2, 1, 3):
        up_x(d).start()
    for d in (2, 1, 3):
        dn_x(d, z).start()
    for d in (2, 1, 3):
        st_y(d).start()
    for d in (2, 1, 3):
        wo_y(d).start()

    def prep(zi, ci, i):
        rows = pl.ds(i * TOK, TOK)
        raw = lat[zi, ci, pl.ds(0, TOK), :].astype(F32)
        mean = jnp.mean(raw * raw, axis=-1, keepdims=True)
        nl = (raw * lax.rsqrt(mean + EPSILON) * lgain[...]).astype(BF16)
        kv = mm(wt[...], nl, NT).astype(BF16)
        va[:, rows] = kv[NOPE_A + NOPE_B : NOPE_A + NOPE_B + V_A]
        vb[:, rows] = kv[NOPE_A + NOPE_B + V_A :]
        rope = lat[zi, ci, pl.ds(TOK, ROPE), :].astype(F32)
        slot = zi * 2 + ci
        cosine = trig[slot, 0:16]
        sine = trig[slot, 16:32]
        square = jnp.sum(rope * rope, axis=0, keepdims=True)

        def one_head(nope, depth, base, dst):
            width = depth - ROPE
            wide = nope.astype(F32)
            total = jnp.sum(wide * wide, axis=0, keepdims=True) + square
            r = lax.rsqrt(total * (1.0 / depth) + EPSILON)
            dst[pl.ds(base, width), :] = (
                wide * r * kgain[pl.ds(base, width), :]
            ).astype(BF16)
            tail = rope * r * kgain[pl.ds(base + width, ROPE), :]
            first = tail[0:16]
            second = tail[16:32]
            dst[pl.ds(base + width, 16), :] = (first * cosine - second * sine).astype(BF16)
            dst[pl.ds(base + width + 16, 16), :] = (
                second * cosine + first * sine
            ).astype(BF16)

        one_head(kv[0:NOPE_A], DEPTH_A, 0, kta)
        one_head(kv[NOPE_A : NOPE_A + NOPE_B], DEPTH_B, DEPTH_A, ktb)
        ka[rows, :] = kta[...].T
        kb[rows, :] = ktb[...].T

    def attend(j, carry):
        queries = qb[j]
        for keys, values, row, scale, lo, width in (
            (ka, va, 0, SCALE_A, 0, V_A),
            (kb, vb, 2, SCALE_B, V_A, V_B),
        ):
            scores = mm(keys[...], queries, NT) * scale
            old = stat[j, row : row + 1]
            new = jnp.maximum(old, jnp.max(scores, axis=0, keepdims=True))
            factor = jnp.exp2(old - new)
            shifted = jnp.exp2(scores - new)
            stat[j, row : row + 1] = new
            stat[j, row + 1 : row + 2] = stat[j, row + 1 : row + 2] * factor + jnp.sum(
                shifted, axis=0, keepdims=True
            )
            part = mm(values[...], shifted.astype(BF16), NN)
            oacc[j, pl.ds(lo, width), :] = oacc[j, pl.ds(lo, width), :] * factor + part
        return carry

    def unit(t, carry):
        odd = lax.rem(t, 2)
        s = lax.div(t + 1, 2)
        edge = lax.div(t, 7) + lax.div(7 - t, 7)
        zm = wrap(z - s, Z)
        zp = wrap(z + s, Z)

        @pl.when(odd == 1)
        def _():
            lat_ring(0, s, zm).wait_recv()

            @pl.when(s < 4)
            def _():
                lat_ring(0, s + 1, zm).start()
                lat_ring(1, s, zp).wait_recv()

                @pl.when(s < 3)
                def _():
                    lat_ring(1, s + 1, zp).start()

                lat_part(1, s, zp).start()

            lat_part(0, s, zm).start()

            dn_ring(0, s, zm).wait_recv()

            @pl.when(s < 4)
            def _():
                dn_ring(0, s + 1, zm).start()
                dn_ring(1, s, zp).wait_recv()

                @pl.when(s < 3)
                def _():
                    dn_ring(1, s + 1, zp).start()

                for d in (2, 1, 3):
                    dn_x(d, zp).start()

            for d in (2, 1, 3):
                dn_x(d, zm).start()

            @pl.when(s == 1)
            def _():
                for d in (1, 2, 3):
                    up_x(d).wait_recv()
                up_ring(0, 1, z).start()
                up_ring(1, 1, z).start()
                up_part(0, 0, z).start()

            @pl.when(s > 1)
            def _():
                su = s - 1
                um = wrap(z - su, Z)
                un = wrap(z + su, Z)
                up_ring(1, su, un).wait_recv()
                up_ring(1, su + 1, un).start()
                up_ring(0, su, um).wait_recv()

                @pl.when(su < 3)
                def _():
                    up_ring(0, su + 1, um).start()

                up_part(0, su, um).start()
                up_part(1, su, un).start()

        @pl.when((odd == 0) | (t == 7))
        def _():
            lat_part(0, s, zm).wait_recv()

        @pl.when((odd == 0) & (t > 0))
        def _():
            lat_part(1, s, zp).wait_recv()

        flip_a = (1 - odd) * (1 - edge)
        flip_b = 1 - odd * (1 - edge)
        prep(zm, c + flip_a * (1 - 2 * c), 0)
        prep(wrap(z + s - 2 * s * edge, Z), c + flip_b * (1 - 2 * c), 1)

        @pl.when(t == 0)
        def _():
            for d in (1, 2, 3):
                q_x(d).wait_recv()

        lax.fori_loop(0, X, attend, 0)
        return carry

    lax.fori_loop(0, 8, unit, 0)

    for j in range(X):
        osend[j, 0:V_A] = (oacc[j, 0:V_A] / stat[j, 1:2]).astype(BF16)
        osend[j, V_A:OUT] = (oacc[j, V_A:OUT] / stat[j, 3:4]).astype(BF16)
    for d in (2, 1, 3):
        s_x(d).start()
        o_x(d).start()
    orecv[x] = osend[x]
    srecv[x] = stat[x]

    up_ring(1, 4, wrap(z + 4, Z)).wait_recv()
    up_part(1, 4, wrap(z + 4, Z)).start()
    dn_part(0).start()
    for d in (1, 2, 3):
        wo_y(d).wait_recv()
        wo_part(d).start()

    for d in (1, 2, 3):
        s_x(d).wait_recv()
        o_x(d).wait_recv()

    for row, lo, width in ((0, 0, V_A), (2, V_A, V_B)):
        peaks = [srecv[i, row : row + 1] for i in range(X)]
        top = functools.reduce(jnp.maximum, peaks)
        shares = [srecv[i, row + 1 : row + 2] * jnp.exp2(peaks[i] - top) for i in range(X)]
        total = shares[0] + shares[1] + shares[2] + shares[3]
        mixed = orecv[0, lo : lo + width].astype(F32) * shares[0]
        for i in range(1, X):
            mixed = mixed + orecv[i, lo : lo + width].astype(F32) * shares[i]
        att[y, pl.ds(lo, width), :] = (mixed / total).astype(BF16)
    for d in (2, 1, 3):
        a_y(d).start()

    for d in (1, 2, 3):
        dn_x_all(d).wait_recv()
        dn_part(d).start()
    for d in (1, 2, 3):
        st_y(d).wait_recv()
        wo_part(d).wait_recv()
    for d in (1, 2, 3):
        a_y(d).wait_recv()

    attended = att[...].reshape(Y * OUT, TOK).T
    squares = jnp.zeros((TOK, 1), F32)
    for n in range(4):
        cols = slice(n * 512, n * 512 + 512)
        weights = wo[:, :, cols].reshape(Y * OUT, 512)
        mixed = mm(attended, weights, NN)
        summed = (st[:, :, cols].reshape(TOK, 512).astype(F32) + mixed).astype(BF16)
        res[:, cols] = summed
        wide = summed.astype(F32)
        squares = squares + jnp.sum(wide * wide, axis=-1, keepdims=True)
    r = lax.rsqrt(squares * (1.0 / D) + EPSILON)
    for n in range(4):
        cols = slice(n * 512, n * 512 + 512)
        nrm[:, cols] = (res[:, cols].astype(F32) * r * ngain[:, cols]).astype(BF16)

    up_part(0, 0, z).wait_recv()
    for s in (1, 2, 3):
        up_part(0, s, z).wait_recv()
    for s in (1, 2, 3, 4):
        up_part(1, s, z).wait_recv()

    for n in range(4):
        cols = slice(n * 256, n * 256 + 256)
        hidden = jnp.maximum(mm(nrm[...], up[:, :, :, :, cols].reshape(D, 256), NN), 0.0)
        act[:, cols] = (hidden * hidden).astype(BF16)

    for d in (0, 1, 2, 3):
        dn_part(d).wait_recv()

    for n in range(4):
        weights = dn[2 * n : 2 * n + 2].reshape(512, FF)
        part = mm(act[...], weights, NT).astype(BF16)
        pb[n] = part.reshape(Y, OWN, 512)
        for d in (2, 1, 3):
            r_y(d, n).start()

    mine = pl.ds(pl.multiple_of(y * OWN, OWN), OWN)
    for n in range(4):
        cols = slice(n * 512, n * 512 + 512)
        total = pb[n, y].astype(F32)
        for d in (1, 2, 3):
            r_y(d, n).wait_recv()
            total = total + rb[wrap(y - d, Y), n].astype(F32)
        out[:, cols] = (res[mine, cols].astype(F32) + total).astype(BF16)

    lat_part(0, 0, z).wait_send()
    up_part(0, 0, z).wait_send()
    for s in (1, 2, 3, 4):
        lat_ring(0, s, z).wait_send()
        lat_part(0, s, z).wait_send()
        dn_ring(0, s, z).wait_send()
        up_ring(1, s, z).wait_send()
        up_part(1, s, z).wait_send()
    for s in (1, 2, 3):
        lat_ring(1, s, z).wait_send()
        lat_part(1, s, z).wait_send()
        dn_ring(1, s, z).wait_send()
        up_ring(0, s, z).wait_send()
        up_part(0, s, z).wait_send()
    for d in (1, 2, 3):
        q_x(d).wait_send()
        up_x(d).wait_send()
        dn_x_all(d).wait_send()
        st_y(d).wait_send()
        wo_y(d).wait_send()
        wo_part(d).wait_send()
        o_x(d).wait_send()
        s_x(d).wait_send()
        a_y(d).wait_send()
        for n in range(4):
            r_y(d, n).wait_send()
    for d in (0, 1, 2, 3):
        dn_part(d).wait_send()


def body(
    stream,
    query_a,
    query_b,
    latent,
    rotary_key,
    latent_gain,
    key_gain_a,
    key_gain_b,
    w_key_a,
    w_value_a,
    w_key_b,
    w_value_b,
    w_out_a,
    w_out_b,
    norm_gain,
    w_up,
    w_down,
):
    sp = lax.axis_index("sp")
    x = (sp // 2) % X
    queries = jnp.concatenate([query_a, query_b], axis=1)
    packed = jnp.concatenate([latent, rotary_key.T], axis=0)
    wt = jnp.concatenate([w_key_a, w_key_b, w_value_a, w_value_b], axis=1).T
    gains = jnp.broadcast_to(
        jnp.concatenate([key_gain_a, key_gain_b])[:, None], (DEPTH_A + DEPTH_B, TOK)
    )
    chunk = jnp.arange(Z, dtype=jnp.int32)[:, None] * 8 + x * 2 + jnp.arange(C, dtype=jnp.int32)
    positions = chunk.reshape(-1, 1) * TOK + jnp.arange(TOK, dtype=jnp.int32)
    freqs = THETA ** (-jnp.arange(ROPE // 2, dtype=F32) / (ROPE // 2))
    angle = positions.astype(F32)[:, None, :] * freqs[:, None]
    trig = jnp.concatenate([jnp.cos(angle), jnp.sin(angle)], axis=1)

    hbm = pl.BlockSpec(memory_space=pltpu.HBM)
    vmem = pl.BlockSpec(memory_space=pltpu.VMEM)
    dma = pltpu.SemaphoreType.DMA
    return pl.pallas_call(
        kernel,
        out_shape=jax.ShapeDtypeStruct((OWN, D), BF16),
        in_specs=[hbm] * 7 + [vmem] * 5,
        out_specs=vmem,
        scratch_shapes=[
            pltpu.VMEM((Z, C, TOK + ROPE, RANK), BF16),
            pltpu.VMEM((X, TOK, DEPTH_A + DEPTH_B), BF16),
            pltpu.VMEM((Z, X, C, 32, FF), BF16),
            pltpu.VMEM((Z, X, C, 32, FF), BF16),
            pltpu.VMEM((Y, OUT, D), BF16),
            pltpu.VMEM((Y, OWN, D), BF16),
            pltpu.VMEM((256, TOK), BF16),
            pltpu.VMEM((256, TOK), BF16),
            pltpu.VMEM((2 * TOK, 256), BF16),
            pltpu.VMEM((2 * TOK, 256), BF16),
            pltpu.VMEM((V_A, 2 * TOK), BF16),
            pltpu.VMEM((V_B, 2 * TOK), BF16),
            pltpu.VMEM((X, OUT, TOK), F32),
            pltpu.VMEM((X, 8, TOK), F32),
            pltpu.VMEM((X, OUT, TOK), BF16),
            pltpu.VMEM((X, OUT, TOK), BF16),
            pltpu.VMEM((X, 8, TOK), F32),
            pltpu.VMEM((Y, OUT, TOK), BF16),
            pltpu.VMEM((TOK, D), BF16),
            pltpu.VMEM((TOK, D), BF16),
            pltpu.VMEM((TOK, FF), BF16),
            pltpu.VMEM((4, Y, OWN, 512), BF16),
            pltpu.VMEM((Y, 4, OWN, 512), BF16),
            dma((7,)),
            dma((2, 5)),
            dma((2, 5)),
            dma((2, 5)),
            dma((2, 5)),
            dma((3,)),
            dma((3,)),
            dma((3,)),
            dma((3,)),
            dma((2, 5)),
            dma((2, 5)),
            dma((2, 5)),
            dma((2, 5)),
            dma((2, 5)),
            dma((2, 5)),
            dma((3,)),
            dma((3,)),
            dma((4,)),
            dma((4,)),
            dma((3,)),
            dma((3,)),
            dma((3,)),
            dma((3,)),
            dma((3,)),
            dma((3,)),
            dma((3,)),
            dma((3,)),
            dma((3,)),
            dma((3,)),
            dma((3,)),
            dma((3,)),
            dma((3, 4)),
            dma((3, 4)),
        ],
        compiler_params=pltpu.CompilerParams(
            collective_id=0, has_side_effects=True, vmem_limit_bytes=56 * 1024 * 1024
        ),
        name="layer",
    )(
        packed,
        queries,
        w_up,
        w_down.T,
        w_out_a,
        w_out_b,
        stream,
        wt,
        latent_gain.reshape(1, RANK),
        gains,
        norm_gain.reshape(1, D),
        trig,
    )


def solution(mesh):
    in_specs = (
        P(("sp", "tp"), None),
        P("sp", "tp"),
        P("sp", "tp"),
        P("sp", None),
        P("sp", None),
        P(),
        P(),
        P(),
        P(None, "tp"),
        P(None, "tp"),
        P(None, "tp"),
        P(None, "tp"),
        P("tp", None),
        P("tp", None),
        P(),
        P("sp", "tp"),
        P("tp", "sp"),
    )
    out_specs = P(("sp", "tp"), None)
    return jax.shard_map(body, mesh=mesh, in_specs=in_specs, out_specs=out_specs, check_vma=False)
```

```python
import functools
import math

import jax
import jax.numpy as jnp
from jax import lax
from jax.experimental import pallas as pl
from jax.experimental.pallas import tpu as pltpu
from jax.sharding import PartitionSpec as P

NOPE_A = 64
V_A = 64
NOPE_B = 128
V_B = 128
ROPE = 32
DEPTH_A = NOPE_A + ROPE
DEPTH_B = NOPE_B + ROPE
KV = NOPE_A + NOPE_B + V_A + V_B
OUT = V_A + V_B
RANK = 256
D = 2048
FF = 1024
TOK = 256
OWN = 64
Z, X, C, Y = 8, 4, 2, 4
EPSILON = 1e-06
THETA = 10000.0
LOG2E = 1.4426950408889634
SCALE_A = DEPTH_A ** (-0.5) * LOG2E
SCALE_B = DEPTH_B ** (-0.5) * LOG2E
NT = (((1,), (1,)), ((), ()))
NN = (((1,), (0,)), ((), ()))
F32 = jnp.float32
BF16 = jnp.bfloat16


def mm(a, b, dims):
    return lax.dot_general(a, b, dims, preferred_element_type=F32)


def kernel(
    lat_in,
    rope_in,
    qa_in,
    qb_in,
    up_in,
    dn_in,
    woa_in,
    wob_in,
    st_in,
    wka_in,
    wkb_in,
    wva_in,
    wvb_in,
    lgain_in,
    gaina_in,
    gainb_in,
    ngain_in,
    out,
    wkb0,
    wvb0,
    lgain,
    gaina0,
    gainb0,
    ngain,
    wt,
    kgain,
    trig,
    s0,
    s1,
    lat,
    qt,
    up,
    dn,
    wo,
    st,
    kta,
    ktb,
    ka,
    kb,
    va,
    vb,
    oacc,
    stat,
    osend,
    orecv,
    srecv,
    att,
    res,
    nrm,
    act,
    pb,
    rb,
    rh,
    loc,
    lat_s,
    lat_r,
    latp_s,
    latp_r,
    q_s,
    q_r,
    upx_s,
    upx_r,
    upz_s,
    upz_r,
    upp_s,
    upp_r,
    dnz_s,
    dnz_r,
    dnx_s,
    dnx_r,
    dnp_s,
    dnp_r,
    st_s,
    st_r,
    wo_s,
    wo_r,
    wop_s,
    wop_r,
    ox_s,
    ox_r,
    sx_s,
    sx_r,
    ay_s,
    ay_r,
    rh_s,
    rh_r,
    rs_s,
    rs_r,
):
    sp = lax.axis_index("sp")
    y = lax.axis_index("tp")
    z = lax.div(sp, 8)
    x = lax.rem(lax.div(sp, 2), 4)
    c = lax.rem(sp, 2)
    oc = 1 - c

    def wrap(v, n):
        return lax.rem(v + 2 * n, n)

    def dev(z_, x_, c_, y_):
        return {"sp": z_ * 8 + x_ * 2 + c_, "tp": y_}

    partner = dev(z, x, oc, y)
    zdev = (dev(wrap(z + 1, Z), x, c, y), dev(wrap(z - 1, Z), x, c, y))
    xdev = [None] + [dev(z, wrap(x + d, X), c, y) for d in (1, 2, 3)]
    ynear = (dev(z, x, c, wrap(y + 1, Y)), dev(z, x, c, wrap(y - 1, Y)))
    ydev = [None] + [dev(z, x, c, wrap(y + d, Y)) for d in (1, 2, 3)]

    def rdma(src, dst, ss, rs, where):
        return pltpu.make_async_remote_copy(
            src_ref=src,
            dst_ref=dst,
            send_sem=ss,
            recv_sem=rs,
            device_id=where,
            device_id_type=pl.DeviceIdType.MESH,
        )

    def same(ref, ss, rs, where):
        return rdma(ref, ref, ss, rs, where)

    pairs = (
        (lat_in, lat.at[z, c, pl.ds(0, TOK)]),
        (rope_in, lat.at[z, c, pl.ds(TOK, ROPE)]),
        (qa_in, qt.at[x, pl.ds(0, DEPTH_A)]),
        (qb_in, qt.at[x, pl.ds(DEPTH_A, DEPTH_B)]),
        (dn_in, dn.at[z, x, c]),
        (up_in, up.at[z, x, c]),
        (st_in, st.at[y]),
        (woa_in, wo.at[y, pl.ds(0, V_A)]),
        (wob_in, wo.at[y, pl.ds(V_A, V_B)]),
        (wka_in, wt.at[pl.ds(0, NOPE_A)]),
        (wva_in, wt.at[pl.ds(NOPE_A + NOPE_B, V_A)]),
        (wkb_in, wkb0),
        (wvb_in, wvb0),
        (lgain_in, lgain),
        (gaina_in, gaina0),
        (gainb_in, gainb0),
        (ngain_in, ngain),
    )
    locals_ = [
        pltpu.make_async_copy(src, dst, loc.at[i]) for i, (src, dst) in enumerate(pairs)
    ]
    for cp in locals_:
        cp.start()

    barrier = pltpu.get_barrier_semaphore()
    for where in [partner, *zdev, *xdev[1:], *ydev[1:]]:
        pl.semaphore_signal(
            barrier, inc=1, device_id=where, device_id_type=pl.DeviceIdType.MESH
        )

    def lat_ring(way, s, zsrc):
        return same(lat.at[zsrc, c], lat_s.at[0], lat_r.at[way, s], zdev[way])

    def lat_part(way, s, zsrc):
        return same(lat.at[zsrc, c], latp_s.at[0], latp_r.at[way, s], partner)

    def q_x(d):
        return same(qt.at[x], q_s.at[0], q_r.at[0], xdev[d])

    def q_all():
        return same(qt.at[pl.ds(0, 3)], q_s.at[0], q_r.at[0], partner)

    def up_x(d):
        return same(up.at[z, x, c], upx_s.at[0], upx_r.at[0], xdev[d])

    def up_x_all():
        return same(up.at[z, pl.ds(0, 3), c], upx_s.at[0], upx_r.at[0], partner)

    def up_ring(way, g, s, zsrc):
        ref = up.at[zsrc, pl.ds(2 * g, 2), c]
        return same(ref, upz_s.at[0], upz_r.at[way, g, s], zdev[way])

    def up_ring_all():
        ref = up.at[pl.ds(0, 7), :, c]
        return same(ref, upz_s.at[0], upz_r.at[0, 0, 0], partner)

    def up_part(g, zsrc):
        return same(up.at[zsrc, pl.ds(2 * g, 2), c], upp_s.at[0], upp_r.at[0], partner)

    def up_part_all():
        return same(up.at[:, :, c], upp_s.at[0], upp_r.at[0], partner)

    def up_start(g):
        up_ring(0, g, 1, z).start()
        up_ring(1, g, 1, z).start()
        up_part(g, z).start()

    def up_step(g, s):
        um = wrap(z - s, Z)
        un = wrap(z + s, Z)
        up_ring(1, g, s, un).wait_recv()
        if s < 4:
            up_ring(1, g, s + 1, un).start()
        up_part(g, un).start()
        if s < 4:
            up_ring(0, g, s, um).wait_recv()
            if s < 3:
                up_ring(0, g, s + 1, um).start()
            up_part(g, um).start()

    def dn_ring(way, s, zsrc):
        return same(dn.at[zsrc, x, c], dnz_s.at[0], dnz_r.at[way, s], zdev[way])

    def dn_x(d, zsrc):
        return same(dn.at[zsrc, x, c], dnx_s.at[0], dnx_r.at[0], xdev[d])

    def dn_x_all():
        return same(dn.at[:, pl.ds(0, 3), c], dnx_s.at[0], dnx_r.at[0], partner)

    def dn_part(d):
        return same(dn.at[:, wrap(x - d, X), c], dnp_s.at[0], dnp_r.at[0], partner)

    def dn_part_all():
        return same(dn.at[:, :, c], dnp_s.at[0], dnp_r.at[0], partner)

    def st_near(k):
        return same(st.at[y], st_s.at[0], st_r.at[k], ynear[k])

    def st_relay(k):
        ref = st.at[wrap(y - 1 + 2 * k, Y), pl.ds(k * (OWN // 2), OWN // 2)]
        return same(ref, st_s.at[1], st_r.at[2], ynear[k])

    def st_relay_all():
        return same(st.at[y], st_s.at[1], st_r.at[2], ynear[0])

    half = pl.ds(pl.multiple_of(c * (D // 2), D // 2), D // 2)

    def wo_near(k):
        return same(wo.at[y, :, half], wo_s.at[0], wo_r.at[k], ynear[k])

    def wo_relay(k):
        cols = pl.ds(pl.multiple_of(c * (D // 2) + k * (D // 4), D // 4), D // 4)
        ref = wo.at[wrap(y - 1 + 2 * k, Y), :, cols]
        return same(ref, wo_s.at[1], wo_r.at[2], ynear[k])

    def wo_relay_all():
        return same(wo.at[y, :, half], wo_s.at[1], wo_r.at[2], ynear[0])

    def wo_part(d):
        return same(wo.at[wrap(y - d, Y), :, half], wop_s.at[0], wop_r.at[0], partner)

    def wo_part_all():
        return same(wo.at[pl.ds(0, 3), :, half], wop_s.at[0], wop_r.at[0], partner)

    def o_x(d):
        return rdma(
            osend.at[wrap(x + d, X)], orecv.at[x], ox_s.at[0], ox_r.at[0], xdev[d]
        )

    def o_all():
        return rdma(
            osend.at[pl.ds(0, 3)], orecv.at[pl.ds(0, 3)], ox_s.at[0], ox_r.at[0], partner
        )

    def s_x(d):
        return rdma(
            stat.at[wrap(x + d, X)], srecv.at[x], sx_s.at[0], sx_r.at[0], xdev[d]
        )

    def s_all():
        return rdma(
            stat.at[pl.ds(0, 3)], srecv.at[pl.ds(0, 3)], sx_s.at[0], sx_r.at[0], partner
        )

    def a_y(d):
        return same(att.at[y], ay_s.at[0], ay_r.at[0], ydev[d])

    def a_all():
        return same(att.at[pl.ds(0, 3)], ay_s.at[0], ay_r.at[0], partner)

    def r_half(k, n):
        return rdma(
            pb.at[n, wrap(y + 2, Y), :, pl.ds(k * 256, 256)],
            rh.at[k, n],
            rh_s.at[k],
            rh_r.at[k, n],
            ynear[k],
        )

    def r_half_all(k):
        return same(rh.at[k], rh_s.at[k], rh_r.at[k, 0], ynear[k])

    def r_full(k, n):
        return rdma(
            pb.at[n, wrap(y + 1 - 2 * k, Y)],
            rb.at[k, n],
            rs_s.at[k],
            rs_r.at[k, n],
            ynear[k],
        )

    def r_full_all(k):
        return same(rb.at[k], rs_s.at[k], rs_r.at[k, 0], ynear[k])

    for cp in locals_[0:4]:
        cp.wait()
    pl.semaphore_wait(barrier, 9)

    lat_ring(0, 1, z).start()
    lat_ring(1, 1, z).start()
    lat_part(0, 0, z).start()
    for d in (1, 3, 2):
        q_x(d).start()
    for cp in locals_[4:9]:
        cp.wait()
    for way in (0, 1):
        dn_ring(way, 1, z).start()
    for d in (1, 3, 2):
        up_x(d).start()
    for d in (1, 3, 2):
        dn_x(d, z).start()
    for k in (0, 1):
        st_near(k).start()
    for k in (0, 1):
        wo_near(k).start()

    kta[...] = jnp.zeros_like(kta)
    ktb[...] = jnp.zeros_like(ktb)
    oacc[...] = jnp.zeros_like(oacc)
    for j in range(X):
        stat[j] = jnp.zeros((8, TOK), F32)
        stat[j, 0:1] = jnp.full((1, TOK), -jnp.inf, F32)
        stat[j, 2:3] = jnp.full((1, TOK), -jnp.inf, F32)
    for cp in locals_[9:]:
        cp.wait()
    wt[NOPE_A : NOPE_A + NOPE_B] = wkb0[...].T
    wt[NOPE_A + NOPE_B + V_A :] = wvb0[...].T
    kgain[0:DEPTH_A] = jnp.broadcast_to(gaina0[...], (TOK, DEPTH_A)).T
    kgain[DEPTH_A : DEPTH_A + DEPTH_B] = jnp.broadcast_to(gainb0[...], (TOK, DEPTH_B)).T
    pair = lax.broadcasted_iota(jnp.int32, (ROPE // 2, TOK), 0).astype(F32)
    freqs = jnp.exp(pair * (-math.log(THETA) / (ROPE // 2)))
    within = lax.broadcasted_iota(jnp.int32, (ROPE // 2, TOK), 1)

    def angles(i, carry):
        chunk = lax.div(i, 2) * 8 + x * 2 + lax.rem(i, 2)
        angle = (within + chunk * TOK).astype(F32) * freqs
        trig[i, 0 : ROPE // 2] = jnp.cos(angle)
        trig[i, ROPE // 2 : ROPE] = jnp.sin(angle)
        return carry

    lax.fori_loop(0, Z * C, angles, 0)

    def prep(zi, ci, i):
        rows = pl.ds(i * TOK, TOK)
        raw = lat[zi, ci, pl.ds(0, TOK), :].astype(F32)
        mean = jnp.mean(raw * raw, axis=-1, keepdims=True)
        nl = (raw * lax.rsqrt(mean + EPSILON) * lgain[...]).astype(BF16)
        kv = mm(wt[...], nl, NT).astype(BF16)
        va[:, rows] = kv[NOPE_A + NOPE_B : NOPE_A + NOPE_B + V_A]
        vb[:, rows] = kv[NOPE_A + NOPE_B + V_A :]
        rope = lat[zi, ci, pl.ds(TOK, ROPE), :].astype(F32)
        slot = zi * 2 + ci
        cosine = trig[slot, 0:16]
        sine = trig[slot, 16:32]
        square = jnp.sum(rope * rope, axis=0, keepdims=True)

        def one_head(nope, depth, base, dst):
            width = depth - ROPE
            wide = nope.astype(F32)
            total = jnp.sum(wide * wide, axis=0, keepdims=True) + square
            r = lax.rsqrt(total * (1.0 / depth) + EPSILON)
            dst[pl.ds(base, width), :] = (
                wide * r * kgain[pl.ds(base, width), :]
            ).astype(BF16)
            tail = rope * r * kgain[pl.ds(base + width, ROPE), :]
            first = tail[0:16]
            second = tail[16:32]
            dst[pl.ds(base + width, 16), :] = (first * cosine - second * sine).astype(BF16)
            dst[pl.ds(base + width + 16, 16), :] = (
                second * cosine + first * sine
            ).astype(BF16)

        one_head(kv[0:NOPE_A], DEPTH_A, 0, kta)
        one_head(kv[NOPE_A : NOPE_A + NOPE_B], DEPTH_B, DEPTH_A, ktb)
        ka[rows, :] = kta[...].T
        kb[rows, :] = ktb[...].T

    peaks = {}

    def score(j):
        held = (s0, s1)[j % 2]
        for h, keys in enumerate((ka, kb)):
            top = None
            for lo in range(0, 2 * TOK, TOK):
                block = mm(keys[lo : lo + TOK], qt[j], NN)
                held[h * 2 * TOK + lo : h * 2 * TOK + lo + TOK] = block
                peak = jnp.max(block, axis=0, keepdims=True)
                top = peak if top is None else jnp.maximum(top, peak)
            peaks[j, h] = top

    def weigh(j):
        held = (s0, s1)[j % 2]
        for h, (values, scale, lo, width) in enumerate(
            ((va, SCALE_A, 0, V_A), (vb, SCALE_B, V_A, V_B))
        ):
            row = 2 * h
            old = stat[j, row : row + 1]
            new = jnp.maximum(old, peaks[j, h] * scale)
            factor = jnp.exp2(old - new)
            shifted = jnp.exp2(held[h * 2 * TOK : (h + 1) * 2 * TOK] * scale - new)
            stat[j, row : row + 1] = new
            stat[j, row + 1 : row + 2] = stat[j, row + 1 : row + 2] * factor + jnp.sum(
                shifted, axis=0, keepdims=True
            )
            part = mm(values[...], shifted.astype(BF16), NN)
            oacc[j, lo : lo + width] = oacc[j, lo : lo + width] * factor + part

    def hook(h):
        hm = wrap(z - h, Z)
        hp = wrap(z + h, Z)
        lat_ring(0, h, hm).wait_recv()

        @pl.when(h < 4)
        def _():
            lat_ring(0, h + 1, hm).start()
            lat_ring(1, h, hp).wait_recv()

            @pl.when(h < 3)
            def _():
                lat_ring(1, h + 1, hp).start()

            lat_part(1, h, hp).start()

        lat_part(0, h, hm).start()
        dn_ring(0, h, hm).wait_recv()

        @pl.when(h < 4)
        def _():
            dn_ring(0, h + 1, hm).start()
            dn_ring(1, h, hp).wait_recv()

            @pl.when(h < 3)
            def _():
                dn_ring(1, h + 1, hp).start()

            for d in (1, 3, 2):
                dn_x(d, hp).start()

        for d in (1, 3, 2):
            dn_x(d, hm).start()

        @pl.when(h == 2)
        def _():
            up_x_all().wait_recv()
            up_start(0)
            for k in (0, 1):
                st_near(k).wait_recv()
                st_relay(k).start()

    def unit(t, carry):
        odd = lax.rem(t, 2)
        s = lax.div(t + 1, 2)
        edge = lax.div(t, 7) + lax.div(7 - t, 7)
        zm = wrap(z - s, Z)
        zp = wrap(z + s, Z)

        @pl.when((odd == 0) | (t == 7))
        def _():
            lat_part(0, s, zm).wait_recv()

        @pl.when((odd == 0) & (t > 0))
        def _():
            lat_part(1, s, zp).wait_recv()

        flip_a = (1 - odd) * (1 - edge)
        flip_b = 1 - odd * (1 - edge)
        prep(zm, c + flip_a * (1 - 2 * c), 0)
        prep(wrap(z + s - 2 * s * edge, Z), c + flip_b * (1 - 2 * c), 1)

        @pl.when(odd == 0)
        def _():
            hook(lax.div(t, 2) + 1)

        @pl.when(t == 0)
        def _():
            q_all().wait_recv()

        score(0)
        for j in range(X):
            if j + 1 < X:
                score(j + 1)
            weigh(j)
        @pl.when(t == 4)
        def _():
            up_step(0, 1)
            up_start(1)
            for k in (0, 1):
                wo_near(k).wait_recv()
                wo_relay(k).start()
            for d in (1, 3):
                wo_part(d).start()

        @pl.when(t == 6)
        def _():
            up_step(0, 2)
            up_step(1, 1)

        return carry

    lax.fori_loop(0, 8, unit, 0)

    for j in range(X):
        osend[j, 0:V_A] = (oacc[j, 0:V_A] / stat[j, 1:2]).astype(BF16)
        osend[j, V_A:OUT] = (oacc[j, V_A:OUT] / stat[j, 3:4]).astype(BF16)
    for d in (2, 1, 3):
        s_x(d).start()
        o_x(d).start()
    orecv[x] = osend[x]
    srecv[x] = stat[x]

    dn_part(0).start()
    up_step(0, 3)
    up_step(1, 2)
    s_all().wait_recv()
    o_all().wait_recv()

    for row, lo, width in ((0, 0, V_A), (2, V_A, V_B)):
        peaks = [srecv[i, row : row + 1] for i in range(X)]
        top = functools.reduce(jnp.maximum, peaks)
        shares = [srecv[i, row + 1 : row + 2] * jnp.exp2(peaks[i] - top) for i in range(X)]
        total = shares[0] + shares[1] + shares[2] + shares[3]
        mixed = orecv[0, lo : lo + width].astype(F32) * shares[0]
        for i in range(1, X):
            mixed = mixed + orecv[i, lo : lo + width].astype(F32) * shares[i]
        att[y, pl.ds(lo, width), :] = (mixed / total).astype(BF16)
    for d in (2, 1, 3):
        a_y(d).start()

    up_step(0, 4)
    up_step(1, 3)
    wo_relay_all().wait_recv()
    wo_part(2).start()
    dn_x_all().wait_recv()
    for d in (1, 2, 3):
        dn_part(d).start()
    st_relay_all().wait_recv()
    wo_part_all().wait_recv()
    a_all().wait_recv()

    attended = att[...].reshape(Y * OUT, TOK).T
    squares = jnp.zeros((TOK, 1), F32)
    for n in range(4):
        cols = slice(n * 512, n * 512 + 512)
        weights = wo[:, :, cols].reshape(Y * OUT, 512)
        mixed = mm(attended, weights, NN)
        summed = (st[:, :, cols].reshape(TOK, 512).astype(F32) + mixed).astype(BF16)
        res[:, cols] = summed
        wide = summed.astype(F32)
        squares = squares + jnp.sum(wide * wide, axis=-1, keepdims=True)
    r = lax.rsqrt(squares * (1.0 / D) + EPSILON)
    for n in range(4):
        cols = slice(n * 512, n * 512 + 512)
        nrm[:, cols] = (res[:, cols].astype(F32) * r * ngain[:, cols]).astype(BF16)

    up_step(1, 4)
    up_part_all().wait_recv()
    for n in range(4):
        cols = slice(n * 256, n * 256 + 256)
        hidden = jnp.maximum(mm(nrm[...], up[:, :, :, :, cols].reshape(D, 256), NN), 0.0)
        act[:, cols] = (hidden * hidden).astype(BF16)

    dn_part_all().wait_recv()

    for n in range(4):
        weights = dn[2 * n : 2 * n + 2].reshape(512, FF)
        part = mm(act[...], weights, NT).astype(BF16)
        pb[n] = part.reshape(Y, OWN, 512)
        for k in (0, 1):
            r_half(k, n).start()

    for n in range(4):
        for k in (0, 1):
            r_half(k, n).wait_recv()
            dest = wrap(y + 1 - 2 * k, Y)
            cols = slice(k * 256, k * 256 + 256)
            pb[n, dest, :, cols] = (
                pb[n, dest, :, cols].astype(F32) + rh[k, n].astype(F32)
            ).astype(BF16)
            r_full(k, n).start()
    mine = pl.ds(pl.multiple_of(y * OWN, OWN), OWN)
    for n in range(4):
        cols = slice(n * 512, n * 512 + 512)
        total = pb[n, y].astype(F32)
        for k in (0, 1):
            r_full(k, n).wait_recv()
            total = total + rb[k, n].astype(F32)
        out[:, cols] = (res[mine, cols].astype(F32) + total).astype(BF16)

    same(lat.at[pl.ds(0, 7), c], lat_s.at[0], lat_r.at[0, 0], partner).wait_send()
    same(lat.at[:, c], latp_s.at[0], latp_r.at[0, 0], partner).wait_send()
    same(dn.at[pl.ds(0, 7), x, c], dnz_s.at[0], dnz_r.at[0, 0], partner).wait_send()
    same(st.at[pl.ds(0, 2)], st_s.at[0], st_r.at[0], partner).wait_send()
    same(wo.at[pl.ds(0, 2), :, half], wo_s.at[0], wo_r.at[0], partner).wait_send()
    q_all().wait_send()
    up_x_all().wait_send()
    up_ring_all().wait_send()
    up_part_all().wait_send()
    dn_x_all().wait_send()
    dn_part_all().wait_send()
    st_relay_all().wait_send()
    wo_relay_all().wait_send()
    wo_part_all().wait_send()
    o_all().wait_send()
    s_all().wait_send()
    a_all().wait_send()
    for k in (0, 1):
        r_half_all(k).wait_send()
        r_full_all(k).wait_send()


def body(
    stream,
    query_a,
    query_b,
    latent,
    rotary_key,
    latent_gain,
    key_gain_a,
    key_gain_b,
    w_key_a,
    w_value_a,
    w_key_b,
    w_value_b,
    w_out_a,
    w_out_b,
    norm_gain,
    w_up,
    w_down,
):
    hbm = pl.BlockSpec(memory_space=pltpu.HBM)
    vmem = pl.BlockSpec(memory_space=pltpu.VMEM)
    dma = pltpu.SemaphoreType.DMA
    return pl.pallas_call(
        kernel,
        out_shape=jax.ShapeDtypeStruct((OWN, D), BF16),
        in_specs=[hbm] * 17,
        out_specs=vmem,
        scratch_shapes=[
            pltpu.VMEM((RANK, NOPE_B), BF16),
            pltpu.VMEM((RANK, V_B), BF16),
            pltpu.VMEM((1, RANK), F32),
            pltpu.VMEM((1, DEPTH_A), F32),
            pltpu.VMEM((1, DEPTH_B), F32),
            pltpu.VMEM((1, D), F32),
            pltpu.VMEM((KV, RANK), BF16),
            pltpu.VMEM((DEPTH_A + DEPTH_B, TOK), F32),
            pltpu.VMEM((Z * C, ROPE, TOK), F32),
            pltpu.VMEM((4 * TOK, TOK), F32),
            pltpu.VMEM((4 * TOK, TOK), F32),
            pltpu.VMEM((Z, C, TOK + ROPE, RANK), BF16),
            pltpu.VMEM((X, TOK, DEPTH_A + DEPTH_B), BF16),
            pltpu.VMEM((Z, X, C, 32, FF), BF16),
            pltpu.VMEM((Z, X, C, 32, FF), BF16),
            pltpu.VMEM((Y, OUT, D), BF16),
            pltpu.VMEM((Y, OWN, D), BF16),
            pltpu.VMEM((256, TOK), BF16),
            pltpu.VMEM((256, TOK), BF16),
            pltpu.VMEM((2 * TOK, 256), BF16),
            pltpu.VMEM((2 * TOK, 256), BF16),
            pltpu.VMEM((V_A, 2 * TOK), BF16),
            pltpu.VMEM((V_B, 2 * TOK), BF16),
            pltpu.VMEM((X, OUT, TOK), F32),
            pltpu.VMEM((X, 8, TOK), F32),
            pltpu.VMEM((X, OUT, TOK), BF16),
            pltpu.VMEM((X, OUT, TOK), BF16),
            pltpu.VMEM((X, 8, TOK), F32),
            pltpu.VMEM((Y, OUT, TOK), BF16),
            pltpu.VMEM((TOK, D), BF16),
            pltpu.VMEM((TOK, D), BF16),
            pltpu.VMEM((TOK, FF), BF16),
            pltpu.VMEM((4, Y, OWN, 512), BF16),
            pltpu.VMEM((2, 4, OWN, 512), BF16),
            pltpu.VMEM((2, 4, OWN, 256), BF16),
            dma((17,)),
            dma((1,)),
            dma((2, 5)),
            dma((1,)),
            dma((2, 5)),
            dma((1,)),
            dma((1,)),
            dma((1,)),
            dma((1,)),
            dma((1,)),
            dma((2, 2, 5)),
            dma((1,)),
            dma((1,)),
            dma((1,)),
            dma((2, 5)),
            dma((1,)),
            dma((1,)),
            dma((1,)),
            dma((1,)),
            dma((2,)),
            dma((3,)),
            dma((2,)),
            dma((3,)),
            dma((1,)),
            dma((1,)),
            dma((1,)),
            dma((1,)),
            dma((1,)),
            dma((1,)),
            dma((1,)),
            dma((1,)),
            dma((2,)),
            dma((2, 4)),
            dma((2,)),
            dma((2, 4)),
        ],
        compiler_params=pltpu.CompilerParams(
            collective_id=0, has_side_effects=True, vmem_limit_bytes=60 * 1024 * 1024,
        ),
        name="layer",
    )(
        latent,
        rotary_key.T,
        query_a.T,
        query_b.T,
        w_up,
        w_down.T,
        w_out_a,
        w_out_b,
        stream,
        w_key_a.T,
        w_key_b,
        w_value_a.T,
        w_value_b,
        latent_gain.reshape(1, RANK),
        key_gain_a.reshape(1, DEPTH_A),
        key_gain_b.reshape(1, DEPTH_B),
        norm_gain.reshape(1, D),
    )


def solution(mesh):
    in_specs = (
        P(("sp", "tp"), None),
        P("sp", "tp"),
        P("sp", "tp"),
        P("sp", None),
        P("sp", None),
        P(),
        P(),
        P(),
        P(None, "tp"),
        P(None, "tp"),
        P(None, "tp"),
        P(None, "tp"),
        P("tp", None),
        P("tp", None),
        P(),
        P("sp", "tp"),
        P("tp", "sp"),
    )
    out_specs = P(("sp", "tp"), None)
    return jax.shard_map(body, mesh=mesh, in_specs=in_specs, out_specs=out_specs, check_vma=False)
```

```python
import functools
import math

import jax
import jax.numpy as jnp
from jax import lax
from jax.experimental import pallas as pl
from jax.experimental.pallas import tpu as pltpu
from jax.sharding import PartitionSpec as P

NOPE_A = 64
V_A = 64
NOPE_B = 128
V_B = 128
ROPE = 32
DEPTH_A = NOPE_A + ROPE
DEPTH_B = NOPE_B + ROPE
KV = NOPE_A + NOPE_B + V_A + V_B
OUT = V_A + V_B
RANK = 256
D = 2048
FF = 1024
TOK = 256
OWN = 64
Z, X, C, Y = 8, 4, 2, 4
EPSILON = 1e-06
THETA = 10000.0
LOG2E = 1.4426950408889634
SCALE_A = DEPTH_A ** (-0.5) * LOG2E
SCALE_B = DEPTH_B ** (-0.5) * LOG2E
NT = (((1,), (1,)), ((), ()))
NN = (((1,), (0,)), ((), ()))
F32 = jnp.float32
BF16 = jnp.bfloat16


def mm(a, b, dims):
    return lax.dot_general(a, b, dims, preferred_element_type=F32)


def kernel(
    lat_in,
    rope_in,
    qa_in,
    qb_in,
    up_in,
    dn_in,
    woa_in,
    wob_in,
    st_in,
    wka_in,
    wkb_in,
    wva_in,
    wvb_in,
    lgain_in,
    gaina_in,
    gainb_in,
    ngain_in,
    out,
    wkb0,
    wvb0,
    lgain,
    gaina0,
    gainb0,
    ngain,
    wt,
    kgain,
    trig,
    s0,
    s1,
    lat,
    qt,
    up,
    dn,
    wo,
    st,
    kta,
    ktb,
    ka,
    kb,
    va,
    vb,
    oacc,
    stat,
    osend,
    orecv,
    srecv,
    att,
    res,
    nrm,
    act,
    pb,
    rb,
    rh,
    loc,
    lat_s,
    lat_r,
    laty_s,
    laty_r,
    latp_s,
    latp_r,
    q_s,
    q_r,
    upx_s,
    upx_r,
    upz_s,
    upz_r,
    upp_s,
    upp_r,
    dnz_s,
    dnz_r,
    dnx_s,
    dnx_r,
    dnr_r,
    dnp_s,
    dnp_r,
    st_s,
    st_r,
    str_r,
    wo_s,
    wo_r,
    wor_r,
    wop_s,
    wop_r,
    ox_s,
    ox_r,
    sx_s,
    sx_r,
    ay_s,
    ay_r,
    rh_s,
    rh_r,
    rs_s,
    rs_r,
):
    sp = lax.axis_index("sp")
    y = lax.axis_index("tp")
    z = lax.div(sp, 8)
    x = lax.rem(lax.div(sp, 2), 4)
    c = lax.rem(sp, 2)
    oc = 1 - c

    def wrap(v, n):
        return lax.rem(v + 2 * n, n)

    def dev(z_, x_, c_, y_):
        return {"sp": z_ * 8 + x_ * 2 + c_, "tp": y_}

    partner = dev(z, x, oc, y)
    zdev = (dev(wrap(z + 1, Z), x, c, y), dev(wrap(z - 1, Z), x, c, y))
    xdev = [None] + [dev(z, wrap(x + d, X), c, y) for d in (1, 2, 3)]
    xnear = (dev(z, wrap(x + 1, X), c, y), dev(z, wrap(x - 1, X), c, y))
    ynear = (dev(z, x, c, wrap(y + 1, Y)), dev(z, x, c, wrap(y - 1, Y)))
    ydev = [None] + [dev(z, x, c, wrap(y + d, Y)) for d in (1, 2, 3)]

    def rdma(src, dst, ss, rs, where):
        return pltpu.make_async_remote_copy(
            src_ref=src,
            dst_ref=dst,
            send_sem=ss,
            recv_sem=rs,
            device_id=where,
            device_id_type=pl.DeviceIdType.MESH,
        )

    def same(ref, ss, rs, where):
        return rdma(ref, ref, ss, rs, where)

    pairs = (
        (lat_in, lat.at[z, c, pl.ds(0, TOK)]),
        (rope_in, lat.at[z, c, pl.ds(TOK, ROPE)]),
        (qa_in, qt.at[x, pl.ds(0, DEPTH_A)]),
        (qb_in, qt.at[x, pl.ds(DEPTH_A, DEPTH_B)]),
        (dn_in, dn.at[z, x, c]),
        (up_in, up.at[z, x, c]),
        (st_in, st.at[y]),
        (woa_in, wo.at[y, pl.ds(0, V_A)]),
        (wob_in, wo.at[y, pl.ds(V_A, V_B)]),
        (wka_in, wt.at[pl.ds(0, NOPE_A)]),
        (wva_in, wt.at[pl.ds(NOPE_A + NOPE_B, V_A)]),
        (wkb_in, wkb0),
        (wvb_in, wvb0),
        (lgain_in, lgain),
        (gaina_in, gaina0),
        (gainb_in, gainb0),
        (ngain_in, ngain),
    )
    locals_ = [
        pltpu.make_async_copy(src, dst, loc.at[i]) for i, (src, dst) in enumerate(pairs)
    ]
    for cp in locals_:
        cp.start()

    barrier = pltpu.get_barrier_semaphore()
    for where in [partner, *zdev, *xdev[1:], *ydev[1:]]:
        pl.semaphore_signal(
            barrier, inc=1, device_id=where, device_id_type=pl.DeviceIdType.MESH
        )

    mine = pl.ds(pl.multiple_of(y * OWN, OWN), OWN)

    def lat_ring(way, s, zsrc):
        for rows in (mine, pl.ds(TOK, ROPE)):
            same(lat.at[zsrc, c, rows], lat_s.at[0], lat_r.at[way, s], zdev[way]).start()

    def lat_ring_wait(way, s):
        ref = lat.at[z, c, pl.ds(0, OWN + ROPE)]
        same(ref, lat_s.at[0], lat_r.at[way, s], zdev[way]).wait_recv()

    def lat_y(way, s, zsrc):
        for d in (1, 3, 2):
            same(lat.at[zsrc, c, mine], laty_s.at[0], laty_r.at[way, s], ydev[d]).start()

    def lat_y_wait(way, s):
        ref = lat.at[z, c, pl.ds(0, 3 * OWN)]
        same(ref, laty_s.at[0], laty_r.at[way, s], partner).wait_recv()

    def lat_part(way, s, zsrc):
        return same(lat.at[zsrc, c], latp_s.at[0], latp_r.at[way, s], partner)

    def q_x(d):
        return same(qt.at[x], q_s.at[0], q_r.at[0], xdev[d])

    def q_all():
        return same(qt.at[pl.ds(0, 3)], q_s.at[0], q_r.at[0], partner)

    def up_x(d):
        return same(up.at[z, x, c], upx_s.at[0], upx_r.at[0], xdev[d])

    def up_x_all():
        return same(up.at[z, pl.ds(0, 3), c], upx_s.at[0], upx_r.at[0], partner)

    def up_ring(way, g, s, zsrc):
        ref = up.at[zsrc, pl.ds(2 * g, 2), c]
        return same(ref, upz_s.at[0], upz_r.at[way, g, s], zdev[way])

    def up_ring_all():
        ref = up.at[pl.ds(0, 7), :, c]
        return same(ref, upz_s.at[0], upz_r.at[0, 0, 0], partner)

    def up_part(g, zsrc):
        return same(up.at[zsrc, pl.ds(2 * g, 2), c], upp_s.at[0], upp_r.at[0], partner)

    def up_part_all():
        return same(up.at[:, :, c], upp_s.at[0], upp_r.at[0], partner)

    def up_start(g):
        up_ring(0, g, 1, z).start()
        up_ring(1, g, 1, z).start()
        up_part(g, z).start()

    def up_step(g, s):
        um = wrap(z - s, Z)
        un = wrap(z + s, Z)
        up_ring(1, g, s, un).wait_recv()
        if s < 4:
            up_ring(1, g, s + 1, un).start()
        up_part(g, un).start()
        if s < 4:
            up_ring(0, g, s, um).wait_recv()
            if s < 3:
                up_ring(0, g, s + 1, um).start()
            up_part(g, um).start()

    def dn_ring(way, s, zsrc):
        return same(dn.at[zsrc, x, c], dnz_s.at[0], dnz_r.at[way, s], zdev[way])

    def dn_near(k, b, zsrc):
        return same(dn.at[zsrc, x, c], dnx_s.at[0], dnx_r.at[k, b], xnear[k])

    def dn_near_wait(k, b):
        ref = dn.at[pl.ds(0, 5 - 2 * b), wrap(x - 1 + 2 * k, X), c]
        same(ref, dnx_s.at[0], dnx_r.at[k, b], xnear[k]).wait_recv()

    def dn_relay(k, zsrc):
        ref = dn.at[zsrc, wrap(x - 1 + 2 * k, X), c, pl.ds(16 * k, 16)]
        return same(ref, dnx_s.at[1], dnr_r.at[0], xnear[k])

    def dn_relay_all():
        return same(dn.at[:, x, c], dnx_s.at[1], dnr_r.at[0], partner)

    def dn_part(d):
        return same(dn.at[:, wrap(x - d, X), c], dnp_s.at[0], dnp_r.at[0], partner)

    def dn_part_all():
        return same(dn.at[:, :, c], dnp_s.at[0], dnp_r.at[0], partner)

    def st_near(k, i):
        rows = pl.ds((OWN // 2) * (k if i == 0 else 1 - k), OWN // 2)
        return same(st.at[y, rows], st_s.at[0], st_r.at[k, i], ynear[k])

    def st_relay(k):
        ref = st.at[wrap(y - 1 + 2 * k, Y), pl.ds(k * (OWN // 2), OWN // 2)]
        return same(ref, st_s.at[1], str_r.at[0], ynear[k])

    def st_relay_all():
        return same(st.at[y], st_s.at[1], str_r.at[0], ynear[0])

    half = pl.ds(pl.multiple_of(c * (D // 2), D // 2), D // 2)

    def wo_cols(k):
        return pl.ds(pl.multiple_of(c * (D // 2) + k * (D // 4), D // 4), D // 4)

    def wo_near(k, i):
        cols = wo_cols(k if i == 0 else 1 - k)
        return same(wo.at[y, :, cols], wo_s.at[0], wo_r.at[k, i], ynear[k])

    def wo_relay(k):
        ref = wo.at[wrap(y - 1 + 2 * k, Y), :, wo_cols(k)]
        return same(ref, wo_s.at[1], wor_r.at[0], ynear[k])

    def wo_relay_all():
        return same(wo.at[y, :, half], wo_s.at[1], wor_r.at[0], ynear[0])

    def wo_part(d):
        return same(wo.at[wrap(y - d, Y), :, half], wop_s.at[0], wop_r.at[0], partner)

    def wo_part_all():
        return same(wo.at[pl.ds(0, 3), :, half], wop_s.at[0], wop_r.at[0], partner)

    def o_x(d):
        return rdma(
            osend.at[wrap(x + d, X)], orecv.at[x], ox_s.at[0], ox_r.at[0], xdev[d]
        )

    def o_all():
        return rdma(
            osend.at[pl.ds(0, 3)], orecv.at[pl.ds(0, 3)], ox_s.at[0], ox_r.at[0], partner
        )

    def s_x(d):
        return rdma(
            stat.at[wrap(x + d, X)], srecv.at[x], sx_s.at[0], sx_r.at[0], xdev[d]
        )

    def s_all():
        return rdma(
            stat.at[pl.ds(0, 3)], srecv.at[pl.ds(0, 3)], sx_s.at[0], sx_r.at[0], partner
        )

    def a_y(d):
        return same(att.at[y], ay_s.at[0], ay_r.at[0], ydev[d])

    def a_all():
        return same(att.at[pl.ds(0, 3)], ay_s.at[0], ay_r.at[0], partner)

    def r_half(k, n):
        return rdma(
            pb.at[n, wrap(y + 2, Y), :, pl.ds(k * 256, 256)],
            rh.at[k, n],
            rh_s.at[k],
            rh_r.at[k, n],
            ynear[k],
        )

    def r_half_all(k):
        return same(rh.at[k], rh_s.at[k], rh_r.at[k, 0], ynear[k])

    def r_full(k, n):
        return rdma(
            pb.at[n, wrap(y + 1 - 2 * k, Y)],
            rb.at[k, n],
            rs_s.at[k],
            rs_r.at[k, n],
            ynear[k],
        )

    def r_full_all(k):
        return same(rb.at[k], rs_s.at[k], rs_r.at[k, 0], ynear[k])

    for cp in locals_[0:4]:
        cp.wait()
    pl.semaphore_wait(barrier, 9)

    lat_ring(0, 1, z)
    lat_ring(1, 1, z)
    lat_part(0, 0, z).start()
    for d in (1, 3, 2):
        q_x(d).start()
    for cp in locals_[4:9]:
        cp.wait()
    for way in (0, 1):
        dn_ring(way, 1, z).start()
    for d in (1, 3, 2):
        up_x(d).start()
    for k in (0, 1):
        dn_near(k, 0, z).start()
        st_near(k, 0).start()

    kta[...] = jnp.zeros_like(kta)
    ktb[...] = jnp.zeros_like(ktb)
    oacc[...] = jnp.zeros_like(oacc)
    for j in range(X):
        stat[j] = jnp.zeros((8, TOK), F32)
        stat[j, 0:1] = jnp.full((1, TOK), -jnp.inf, F32)
        stat[j, 2:3] = jnp.full((1, TOK), -jnp.inf, F32)
    for cp in locals_[9:]:
        cp.wait()
    wt[NOPE_A : NOPE_A + NOPE_B] = wkb0[...].T
    wt[NOPE_A + NOPE_B + V_A :] = wvb0[...].T
    kgain[0:DEPTH_A] = jnp.broadcast_to(gaina0[...], (TOK, DEPTH_A)).T
    kgain[DEPTH_A : DEPTH_A + DEPTH_B] = jnp.broadcast_to(gainb0[...], (TOK, DEPTH_B)).T
    pair = lax.broadcasted_iota(jnp.int32, (ROPE // 2, TOK), 0).astype(F32)
    freqs = jnp.exp(pair * (-math.log(THETA) / (ROPE // 2)))
    within = lax.broadcasted_iota(jnp.int32, (ROPE // 2, TOK), 1)

    def angles(i, carry):
        chunk = lax.div(i, 2) * 8 + x * 2 + lax.rem(i, 2)
        angle = (within + chunk * TOK).astype(F32) * freqs
        trig[i, 0 : ROPE // 2] = jnp.cos(angle)
        trig[i, ROPE // 2 : ROPE] = jnp.sin(angle)
        return carry

    lax.fori_loop(0, Z * C, angles, 0)

    def prep(zi, ci, i):
        rows = pl.ds(i * TOK, TOK)
        raw = lat[zi, ci, pl.ds(0, TOK), :].astype(F32)
        mean = jnp.mean(raw * raw, axis=-1, keepdims=True)
        nl = (raw * lax.rsqrt(mean + EPSILON) * lgain[...]).astype(BF16)
        kv = mm(wt[...], nl, NT).astype(BF16)
        va[:, rows] = kv[NOPE_A + NOPE_B : NOPE_A + NOPE_B + V_A]
        vb[:, rows] = kv[NOPE_A + NOPE_B + V_A :]
        rope = lat[zi, ci, pl.ds(TOK, ROPE), :].astype(F32)
        slot = zi * 2 + ci
        cosine = trig[slot, 0:16]
        sine = trig[slot, 16:32]
        square = jnp.sum(rope * rope, axis=0, keepdims=True)

        def one_head(nope, depth, base, dst):
            width = depth - ROPE
            wide = nope.astype(F32)
            total = jnp.sum(wide * wide, axis=0, keepdims=True) + square
            r = lax.rsqrt(total * (1.0 / depth) + EPSILON)
            dst[pl.ds(base, width), :] = (
                wide * r * kgain[pl.ds(base, width), :]
            ).astype(BF16)
            tail = rope * r * kgain[pl.ds(base + width, ROPE), :]
            first = tail[0:16]
            second = tail[16:32]
            dst[pl.ds(base + width, 16), :] = (first * cosine - second * sine).astype(BF16)
            dst[pl.ds(base + width + 16, 16), :] = (
                second * cosine + first * sine
            ).astype(BF16)

        one_head(kv[0:NOPE_A], DEPTH_A, 0, kta)
        one_head(kv[NOPE_A : NOPE_A + NOPE_B], DEPTH_B, DEPTH_A, ktb)
        ka[rows, :] = kta[...].T
        kb[rows, :] = ktb[...].T

    peaks = {}

    def score(j):
        held = (s0, s1)[j % 2]
        for h, keys in enumerate((ka, kb)):
            top = None
            for lo in range(0, 2 * TOK, TOK):
                block = mm(keys[lo : lo + TOK], qt[j], NN)
                held[h * 2 * TOK + lo : h * 2 * TOK + lo + TOK] = block
                peak = jnp.max(block, axis=0, keepdims=True)
                top = peak if top is None else jnp.maximum(top, peak)
            peaks[j, h] = top

    def weigh(j):
        held = (s0, s1)[j % 2]
        for h, (values, scale, lo, width) in enumerate(
            ((va, SCALE_A, 0, V_A), (vb, SCALE_B, V_A, V_B))
        ):
            row = 2 * h
            old = stat[j, row : row + 1]
            new = jnp.maximum(old, peaks[j, h] * scale)
            factor = jnp.exp2(old - new)
            shifted = jnp.exp2(held[h * 2 * TOK : (h + 1) * 2 * TOK] * scale - new)
            stat[j, row : row + 1] = new
            stat[j, row + 1 : row + 2] = stat[j, row + 1 : row + 2] * factor + jnp.sum(
                shifted, axis=0, keepdims=True
            )
            part = mm(values[...], shifted.astype(BF16), NN)
            oacc[j, lo : lo + width] = oacc[j, lo : lo + width] * factor + part

    def lat_step(s):
        zm = wrap(z - s, Z)
        zp = wrap(z + s, Z)
        lat_ring_wait(0, s)
        if s < 4:
            lat_ring(0, s + 1, zm)
            lat_ring_wait(1, s)
            if s < 3:
                lat_ring(1, s + 1, zp)
            lat_y(1, s, zp)
        lat_y(0, s, zm)

    def lat_spread(s):
        lat_y_wait(0, s)
        lat_part(0, s, wrap(z - s, Z)).start()
        if s < 4:
            lat_y_wait(1, s)
            lat_part(1, s, wrap(z + s, Z)).start()

    def dn_step(s):
        zm = wrap(z - s, Z)
        zp = wrap(z + s, Z)
        bulk = s // 3
        dn_ring(0, s, zm).wait_recv()
        if s < 4:
            dn_ring(0, s + 1, zm).start()
            dn_ring(1, s, zp).wait_recv()
            if s < 3:
                dn_ring(1, s + 1, zp).start()
        for k in (0, 1):
            dn_near(k, bulk, zm).start()
            if s < 4:
                dn_near(k, bulk, zp).start()

    def dn_forward(bulk):
        for k in (0, 1):
            dn_near_wait(k, bulk)
            for s in ((0, 1, 2), (3, 4))[bulk]:
                dn_relay(k, wrap(z - s, Z)).start()
                if 0 < s < 4:
                    dn_relay(k, wrap(z + s, Z)).start()

    def before(t):
        if t == 0:
            lat_step(1)
            dn_step(1)
            lat_step(2)
            for k in (0, 1):
                st_near(k, 1).start()
            dn_step(2)
            lat_spread(1)
        elif t == 1:
            lat_step(3)
            dn_step(3)
            up_x_all().wait_recv()
            up_start(0)
            up_start(1)
            for k in (0, 1):
                wo_near(k, 0).start()
        elif t == 2:
            lat_spread(2)
        elif t == 3:
            lat_step(4)
            dn_step(4)
            for k in (0, 1):
                wo_near(k, 1).start()
        elif t == 4:
            lat_spread(3)
        elif t == 6:
            lat_spread(4)

    def after(t):
        if t == 3:
            up_step(0, 1)
        elif t == 4:
            up_step(1, 1)
            for k in (0, 1):
                st_near(k, 0).wait_recv()
                st_relay(k).start()
            dn_forward(0)
        elif t == 6:
            up_step(0, 2)
            for k in (0, 1):
                wo_near(k, 0).wait_recv()
                wo_relay(k).start()
        elif t == 7:
            up_step(1, 2)
            dn_forward(1)
            for k in (0, 1):
                wo_near(k, 1).wait_recv()
                wo_part(1 + 2 * k).start()

    def at(t, fn, times):
        for i in times:
            pl.when(t == i)(functools.partial(fn, i))

    def unit(t, carry):
        odd = lax.rem(t, 2)
        s = lax.div(t + 1, 2)
        edge = lax.div(t, 7) + lax.div(7 - t, 7)
        zm = wrap(z - s, Z)
        zp = wrap(z + s, Z)

        @pl.when((odd == 0) | (t == 7))
        def _():
            lat_part(0, s, zm).wait_recv()

        @pl.when((odd == 0) & (t > 0))
        def _():
            lat_part(1, s, zp).wait_recv()

        flip_a = (1 - odd) * (1 - edge)
        flip_b = 1 - odd * (1 - edge)
        prep(zm, c + flip_a * (1 - 2 * c), 0)
        prep(wrap(z + s - 2 * s * edge, Z), c + flip_b * (1 - 2 * c), 1)

        at(t, before, (0, 1, 2, 3, 4, 6))
        @pl.when(t == 0)
        def _():
            q_all().wait_recv()

        score(0)
        for j in range(X):
            if j + 1 < X:
                score(j + 1)
            weigh(j)
        at(t, after, (3, 4, 6, 7))
        return carry

    lax.fori_loop(0, 8, unit, 0)

    for j in range(X):
        osend[j, 0:V_A] = (oacc[j, 0:V_A] / stat[j, 1:2]).astype(BF16)
        osend[j, V_A:OUT] = (oacc[j, V_A:OUT] / stat[j, 3:4]).astype(BF16)
    for d in (2, 1, 3):
        s_x(d).start()
        o_x(d).start()
    orecv[x] = osend[x]
    srecv[x] = stat[x]

    for d in (0, 1, 3):
        dn_part(d).start()
    up_step(0, 3)
    s_all().wait_recv()
    o_all().wait_recv()

    for row, lo, width in ((0, 0, V_A), (2, V_A, V_B)):
        peaks = [srecv[i, row : row + 1] for i in range(X)]
        top = functools.reduce(jnp.maximum, peaks)
        shares = [srecv[i, row + 1 : row + 2] * jnp.exp2(peaks[i] - top) for i in range(X)]
        total = shares[0] + shares[1] + shares[2] + shares[3]
        mixed = orecv[0, lo : lo + width].astype(F32) * shares[0]
        for i in range(1, X):
            mixed = mixed + orecv[i, lo : lo + width].astype(F32) * shares[i]
        att[y, pl.ds(lo, width), :] = (mixed / total).astype(BF16)
    for d in (2, 1, 3):
        a_y(d).start()

    up_step(1, 3)
    up_step(0, 4)
    wo_relay_all().wait_recv()
    wo_part(2).start()
    dn_relay_all().wait_recv()
    dn_part(2).start()
    for k in (0, 1):
        st_near(k, 1).wait_recv()
    st_relay_all().wait_recv()
    wo_part_all().wait_recv()
    a_all().wait_recv()

    attended = att[...].reshape(Y * OUT, TOK).T
    squares = jnp.zeros((TOK, 1), F32)
    for n in range(4):
        cols = slice(n * 512, n * 512 + 512)
        weights = wo[:, :, cols].reshape(Y * OUT, 512)
        mixed = mm(attended, weights, NN)
        summed = (st[:, :, cols].reshape(TOK, 512).astype(F32) + mixed).astype(BF16)
        res[:, cols] = summed
        wide = summed.astype(F32)
        squares = squares + jnp.sum(wide * wide, axis=-1, keepdims=True)
    r = lax.rsqrt(squares * (1.0 / D) + EPSILON)
    for n in range(4):
        cols = slice(n * 512, n * 512 + 512)
        nrm[:, cols] = (res[:, cols].astype(F32) * r * ngain[:, cols]).astype(BF16)

    up_step(1, 4)
    up_part_all().wait_recv()
    for n in range(4):
        cols = slice(n * 256, n * 256 + 256)
        hidden = jnp.maximum(mm(nrm[...], up[:, :, :, :, cols].reshape(D, 256), NN), 0.0)
        act[:, cols] = (hidden * hidden).astype(BF16)

    dn_part_all().wait_recv()

    for n in range(4):
        weights = dn[2 * n : 2 * n + 2].reshape(512, FF)
        part = mm(act[...], weights, NT).astype(BF16)
        pb[n] = part.reshape(Y, OWN, 512)
        for k in (0, 1):
            r_half(k, n).start()

    for n in range(4):
        for k in (0, 1):
            r_half(k, n).wait_recv()
            dest = wrap(y + 1 - 2 * k, Y)
            cols = slice(k * 256, k * 256 + 256)
            pb[n, dest, :, cols] = (
                pb[n, dest, :, cols].astype(F32) + rh[k, n].astype(F32)
            ).astype(BF16)
            r_full(k, n).start()
    for n in range(4):
        cols = slice(n * 512, n * 512 + 512)
        total = pb[n, y].astype(F32)
        for k in (0, 1):
            r_full(k, n).wait_recv()
            total = total + rb[k, n].astype(F32)
        out[:, cols] = (res[mine, cols].astype(F32) + total).astype(BF16)

    same(lat.at[pl.ds(0, 7), c, pl.ds(0, OWN + ROPE)], lat_s.at[0], lat_r.at[0, 0], partner).wait_send()
    same(
        lat.at[pl.ds(0, 7), c, pl.ds(0, 3 * OWN)], laty_s.at[0], laty_r.at[0, 0], partner
    ).wait_send()
    same(lat.at[:, c], latp_s.at[0], latp_r.at[0, 0], partner).wait_send()
    same(dn.at[pl.ds(0, 7), x, c], dnz_s.at[0], dnz_r.at[0, 0], partner).wait_send()
    same(st.at[pl.ds(0, 2)], st_s.at[0], st_r.at[0], partner).wait_send()
    same(wo.at[pl.ds(0, 2), :, half], wo_s.at[0], wo_r.at[0], partner).wait_send()
    q_all().wait_send()
    up_x_all().wait_send()
    up_ring_all().wait_send()
    up_part_all().wait_send()
    same(dn.at[:, pl.ds(0, 2), c], dnx_s.at[0], dnx_r.at[0, 0], partner).wait_send()
    dn_relay_all().wait_send()
    dn_part_all().wait_send()
    st_relay_all().wait_send()
    wo_relay_all().wait_send()
    wo_part_all().wait_send()
    o_all().wait_send()
    s_all().wait_send()
    a_all().wait_send()
    for k in (0, 1):
        r_half_all(k).wait_send()
        r_full_all(k).wait_send()


def body(
    stream,
    query_a,
    query_b,
    latent,
    rotary_key,
    latent_gain,
    key_gain_a,
    key_gain_b,
    w_key_a,
    w_value_a,
    w_key_b,
    w_value_b,
    w_out_a,
    w_out_b,
    norm_gain,
    w_up,
    w_down,
):
    hbm = pl.BlockSpec(memory_space=pltpu.HBM)
    vmem = pl.BlockSpec(memory_space=pltpu.VMEM)
    dma = pltpu.SemaphoreType.DMA
    return pl.pallas_call(
        kernel,
        out_shape=jax.ShapeDtypeStruct((OWN, D), BF16),
        in_specs=[hbm] * 17,
        out_specs=vmem,
        scratch_shapes=[
            pltpu.VMEM((RANK, NOPE_B), BF16),
            pltpu.VMEM((RANK, V_B), BF16),
            pltpu.VMEM((1, RANK), F32),
            pltpu.VMEM((1, DEPTH_A), F32),
            pltpu.VMEM((1, DEPTH_B), F32),
            pltpu.VMEM((1, D), F32),
            pltpu.VMEM((KV, RANK), BF16),
            pltpu.VMEM((DEPTH_A + DEPTH_B, TOK), F32),
            pltpu.VMEM((Z * C, ROPE, TOK), F32),
            pltpu.VMEM((4 * TOK, TOK), F32),
            pltpu.VMEM((4 * TOK, TOK), F32),
            pltpu.VMEM((Z, C, TOK + ROPE, RANK), BF16),
            pltpu.VMEM((X, TOK, DEPTH_A + DEPTH_B), BF16),
            pltpu.VMEM((Z, X, C, 32, FF), BF16),
            pltpu.VMEM((Z, X, C, 32, FF), BF16),
            pltpu.VMEM((Y, OUT, D), BF16),
            pltpu.VMEM((Y, OWN, D), BF16),
            pltpu.VMEM((256, TOK), BF16),
            pltpu.VMEM((256, TOK), BF16),
            pltpu.VMEM((2 * TOK, 256), BF16),
            pltpu.VMEM((2 * TOK, 256), BF16),
            pltpu.VMEM((V_A, 2 * TOK), BF16),
            pltpu.VMEM((V_B, 2 * TOK), BF16),
            pltpu.VMEM((X, OUT, TOK), F32),
            pltpu.VMEM((X, 8, TOK), F32),
            pltpu.VMEM((X, OUT, TOK), BF16),
            pltpu.VMEM((X, OUT, TOK), BF16),
            pltpu.VMEM((X, 8, TOK), F32),
            pltpu.VMEM((Y, OUT, TOK), BF16),
            pltpu.VMEM((TOK, D), BF16),
            pltpu.VMEM((TOK, D), BF16),
            pltpu.VMEM((TOK, FF), BF16),
            pltpu.VMEM((4, Y, OWN, 512), BF16),
            pltpu.VMEM((2, 4, OWN, 512), BF16),
            pltpu.VMEM((2, 4, OWN, 256), BF16),
            dma((17,)),
            dma((1,)),
            dma((2, 5)),
            dma((1,)),
            dma((2, 5)),
            dma((1,)),
            dma((2, 5)),
            dma((1,)),
            dma((1,)),
            dma((1,)),
            dma((1,)),
            dma((1,)),
            dma((2, 2, 5)),
            dma((1,)),
            dma((1,)),
            dma((1,)),
            dma((2, 5)),
            dma((2,)),
            dma((2, 2)),
            dma((1,)),
            dma((1,)),
            dma((1,)),
            dma((2,)),
            dma((2, 2)),
            dma((1,)),
            dma((2,)),
            dma((2, 2)),
            dma((1,)),
            dma((1,)),
            dma((1,)),
            dma((1,)),
            dma((1,)),
            dma((1,)),
            dma((1,)),
            dma((1,)),
            dma((1,)),
            dma((2,)),
            dma((2, 4)),
            dma((2,)),
            dma((2, 4)),
        ],
        compiler_params=pltpu.CompilerParams(
            collective_id=0, has_side_effects=True, vmem_limit_bytes=60 * 1024 * 1024,
        ),
        name="layer",
    )(
        latent,
        rotary_key.T,
        query_a.T,
        query_b.T,
        w_up,
        w_down.T,
        w_out_a,
        w_out_b,
        stream,
        w_key_a.T,
        w_key_b,
        w_value_a.T,
        w_value_b,
        latent_gain.reshape(1, RANK),
        key_gain_a.reshape(1, DEPTH_A),
        key_gain_b.reshape(1, DEPTH_B),
        norm_gain.reshape(1, D),
    )


def solution(mesh):
    in_specs = (
        P(("sp", "tp"), None),
        P("sp", "tp"),
        P("sp", "tp"),
        P("sp", None),
        P("sp", None),
        P(),
        P(),
        P(),
        P(None, "tp"),
        P(None, "tp"),
        P(None, "tp"),
        P(None, "tp"),
        P("tp", None),
        P("tp", None),
        P(),
        P("sp", "tp"),
        P("tp", "sp"),
    )
    out_specs = P(("sp", "tp"), None)
    return jax.shard_map(body, mesh=mesh, in_specs=in_specs, out_specs=out_specs, check_vma=False)
```

```python
import functools
import math

import jax
import jax.numpy as jnp
from jax import lax
from jax.experimental import pallas as pl
from jax.experimental.pallas import tpu as pltpu
from jax.sharding import PartitionSpec as P

NOPE_A = 64
V_A = 64
NOPE_B = 128
V_B = 128
ROPE = 32
DEPTH_A = NOPE_A + ROPE
DEPTH_B = NOPE_B + ROPE
KV = NOPE_A + NOPE_B + V_A + V_B
OUT = V_A + V_B
RANK = 256
D = 2048
FF = 1024
TOK = 256
OWN = 64
Z, X, C, Y = 8, 4, 2, 4
SETS = ((0,), (1, 3), (2,))
EPSILON = 1e-06
THETA = 10000.0
LOG2E = 1.4426950408889634
SCALE_A = DEPTH_A ** (-0.5) * LOG2E
SCALE_B = DEPTH_B ** (-0.5) * LOG2E
NT = (((1,), (1,)), ((), ()))
NN = (((1,), (0,)), ((), ()))
F32 = jnp.float32
BF16 = jnp.bfloat16


def mm(a, b, dims):
    return lax.dot_general(a, b, dims, preferred_element_type=F32)


def kernel(
    lat_in,
    rope_in,
    qa_in,
    qb_in,
    up_in,
    dn_in,
    woa_in,
    wob_in,
    st_in,
    wka_in,
    wkb_in,
    wva_in,
    wvb_in,
    lgain_in,
    gaina_in,
    gainb_in,
    ngain_in,
    out,
    wkb0,
    wvb0,
    lgain,
    gaina0,
    gainb0,
    ngain,
    wt,
    kgain,
    trig,
    s0,
    s1,
    lat,
    qt,
    up,
    dn,
    wo,
    st,
    kta,
    ktb,
    ka,
    kb,
    va,
    vb,
    vna,
    vnb,
    oacc,
    stat,
    osend,
    orecv,
    srecv,
    att,
    res,
    nrm,
    act,
    pb,
    rb,
    rh,
    ob,
    loc,
    lat_s,
    lat_r,
    laty_s,
    laty_r,
    latp_s,
    latp_r,
    q_s,
    q_r,
    upx_s,
    upx_r,
    upz_s,
    upz_r,
    upp_s,
    upp_r,
    dnz_s,
    dnz_r,
    dnx_s,
    dnx_r,
    dnr_r,
    dnp_s,
    dnp_r,
    st_s,
    st_r,
    str_r,
    wo_s,
    wo_r,
    wor_r,
    wop_s,
    wop_r,
    ox_s,
    ox_r,
    sx_s,
    sx_r,
    ay_s,
    ay_r,
    rh_s,
    rh_r,
    rs_s,
    rs_r,
):
    sp = lax.axis_index("sp")
    y = lax.axis_index("tp")
    z = lax.div(sp, 8)
    x = lax.rem(lax.div(sp, 2), 4)
    c = lax.rem(sp, 2)
    oc = 1 - c

    def wrap(v, n):
        return lax.rem(v + 2 * n, n)

    def dev(z_, x_, c_, y_):
        return {"sp": z_ * 8 + x_ * 2 + c_, "tp": y_}

    partner = dev(z, x, oc, y)
    zdev = (dev(wrap(z + 1, Z), x, c, y), dev(wrap(z - 1, Z), x, c, y))
    xdev = [None] + [dev(z, wrap(x + d, X), c, y) for d in (1, 2, 3)]
    xnear = (dev(z, wrap(x + 1, X), c, y), dev(z, wrap(x - 1, X), c, y))
    ynear = (dev(z, x, c, wrap(y + 1, Y)), dev(z, x, c, wrap(y - 1, Y)))
    ydev = [None] + [dev(z, x, c, wrap(y + d, Y)) for d in (1, 2, 3)]

    def rdma(src, dst, ss, rs, where):
        return pltpu.make_async_remote_copy(
            src_ref=src,
            dst_ref=dst,
            send_sem=ss,
            recv_sem=rs,
            device_id=where,
            device_id_type=pl.DeviceIdType.MESH,
        )

    def same(ref, ss, rs, where):
        return rdma(ref, ref, ss, rs, where)

    pairs = (
        (lat_in, lat.at[z, c, pl.ds(0, TOK)]),
        (rope_in, lat.at[z, c, pl.ds(TOK, ROPE)]),
        (qa_in, qt.at[x, pl.ds(0, DEPTH_A)]),
        (qb_in, qt.at[x, pl.ds(DEPTH_A, DEPTH_B)]),
        (dn_in, dn.at[z, x, c]),
        (up_in, up.at[z, x, c]),
        (st_in, st.at[y]),
        (woa_in, wo.at[y, pl.ds(0, V_A)]),
        (wob_in, wo.at[y, pl.ds(V_A, V_B)]),
        (wka_in, wt.at[pl.ds(0, NOPE_A)]),
        (wva_in, wt.at[pl.ds(NOPE_A + NOPE_B, V_A)]),
        (wkb_in, wkb0),
        (wvb_in, wvb0),
        (lgain_in, lgain),
        (gaina_in, gaina0),
        (gainb_in, gainb0),
        (ngain_in, ngain),
    )
    locals_ = [
        pltpu.make_async_copy(src, dst, loc.at[i]) for i, (src, dst) in enumerate(pairs)
    ]
    for cp in locals_:
        cp.start()

    barrier = pltpu.get_barrier_semaphore()
    for where in [partner, *zdev, *xdev[1:], *ydev[1:]]:
        pl.semaphore_signal(
            barrier, inc=1, device_id=where, device_id_type=pl.DeviceIdType.MESH
        )

    mine = pl.ds(pl.multiple_of(y * OWN, OWN), OWN)

    def lat_ring(way, s, zsrc):
        for rows in (mine, pl.ds(TOK, ROPE)):
            same(lat.at[zsrc, c, rows], lat_s.at[0], lat_r.at[way, s], zdev[way]).start()

    def lat_ring_wait(way, s):
        ref = lat.at[z, c, pl.ds(0, OWN + ROPE)]
        same(ref, lat_s.at[0], lat_r.at[way, s], zdev[way]).wait_recv()

    def lat_y(way, s, zsrc):
        for d in (1, 3, 2):
            same(lat.at[zsrc, c, mine], laty_s.at[0], laty_r.at[way, s], ydev[d]).start()

    def lat_y_wait(way, s):
        ref = lat.at[z, c, pl.ds(0, 3 * OWN)]
        same(ref, laty_s.at[0], laty_r.at[way, s], partner).wait_recv()

    def lat_part(way, s, zsrc):
        return same(lat.at[zsrc, c], latp_s.at[0], latp_r.at[way, s], partner)

    def q_x(d):
        return same(qt.at[x], q_s.at[0], q_r.at[d - 1], xdev[d])

    def q_all():
        return same(qt.at[pl.ds(0, 3)], q_s.at[0], q_r.at[0], partner)

    def q_wait(d):
        q_x(d).wait_recv()

    def up_x(d):
        return same(up.at[z, x, c], upx_s.at[0], upx_r.at[0], xdev[d])

    def up_x_all():
        return same(up.at[z, pl.ds(0, 3), c], upx_s.at[0], upx_r.at[0], partner)

    def up_hop(way, g, s, zsrc):
        for d in SETS[g]:
            ref = up.at[zsrc, wrap(x - d, X), c]
            same(ref, upz_s.at[0], upz_r.at[way, g, s], zdev[way]).start()

    def up_hop_wait(way, g, s):
        ref = up.at[z, pl.ds(0, len(SETS[g])), c]
        same(ref, upz_s.at[0], upz_r.at[way, g, s], zdev[way]).wait_recv()

    def up_ring_all():
        ref = up.at[pl.ds(0, 7), :, c]
        return same(ref, upz_s.at[0], upz_r.at[0, 0, 0], partner)

    def up_part(g, zsrc):
        for d in SETS[g]:
            ref = up.at[zsrc, wrap(x - d, X), c]
            same(ref, upp_s.at[0], upp_r.at[0], partner).start()

    def up_part_all():
        return same(up.at[:, :, c], upp_s.at[0], upp_r.at[0], partner)

    def up_start(g):
        up_hop(0, g, 1, z)
        up_hop(1, g, 1, z)
        up_part(g, z)

    def up_step(g, s):
        um = wrap(z - s, Z)
        un = wrap(z + s, Z)
        up_hop_wait(1, g, s)
        if s < 4:
            up_hop(1, g, s + 1, un)
        up_part(g, un)
        if s < 4:
            up_hop_wait(0, g, s)
            if s < 3:
                up_hop(0, g, s + 1, um)
            up_part(g, um)

    def dn_ring(way, s, zsrc):
        return same(dn.at[zsrc, x, c], dnz_s.at[0], dnz_r.at[way, s], zdev[way])

    def dn_near(k, b, zsrc):
        return same(dn.at[zsrc, x, c], dnx_s.at[0], dnx_r.at[k, b], xnear[k])

    def dn_near_wait(k, b):
        ref = dn.at[pl.ds(0, 5 - 2 * b), wrap(x - 1 + 2 * k, X), c]
        same(ref, dnx_s.at[0], dnx_r.at[k, b], xnear[k]).wait_recv()

    def dn_relay(k, zsrc):
        ref = dn.at[zsrc, wrap(x - 1 + 2 * k, X), c, pl.ds(16 * k, 16)]
        return same(ref, dnx_s.at[1], dnr_r.at[0], xnear[k])

    def dn_relay_all():
        return same(dn.at[:, x, c], dnx_s.at[1], dnr_r.at[0], partner)

    def dn_part(d):
        return same(dn.at[:, wrap(x - d, X), c], dnp_s.at[0], dnp_r.at[0], partner)

    def dn_part_all():
        return same(dn.at[:, :, c], dnp_s.at[0], dnp_r.at[0], partner)

    def st_near(k, i):
        rows = pl.ds((OWN // 2) * (k if i == 0 else 1 - k), OWN // 2)
        return same(st.at[y, rows], st_s.at[0], st_r.at[k, i], ynear[k])

    def st_relay(k):
        ref = st.at[wrap(y - 1 + 2 * k, Y), pl.ds(k * (OWN // 2), OWN // 2)]
        return same(ref, st_s.at[1], str_r.at[0], ynear[k])

    def st_relay_all():
        return same(st.at[y], st_s.at[1], str_r.at[0], ynear[0])

    half = pl.ds(pl.multiple_of(c * (D // 2), D // 2), D // 2)

    def wo_cols(k):
        return pl.ds(pl.multiple_of(c * (D // 2) + k * (D // 4), D // 4), D // 4)

    def wo_near(k, i):
        cols = wo_cols(k if i == 0 else 1 - k)
        return same(wo.at[y, :, cols], wo_s.at[0], wo_r.at[k, i], ynear[k])

    def wo_relay(k):
        ref = wo.at[wrap(y - 1 + 2 * k, Y), :, wo_cols(k)]
        return same(ref, wo_s.at[1], wor_r.at[0], ynear[k])

    def wo_relay_all():
        return same(wo.at[y, :, half], wo_s.at[1], wor_r.at[0], ynear[0])

    def wo_part(d):
        return same(wo.at[wrap(y - d, Y), :, half], wop_s.at[0], wop_r.at[0], partner)

    def wo_part_all():
        return same(wo.at[pl.ds(0, 3), :, half], wop_s.at[0], wop_r.at[0], partner)

    def o_x(d):
        return rdma(
            osend.at[wrap(x + d, X)], orecv.at[x], ox_s.at[0], ox_r.at[0], xdev[d]
        )

    def o_all():
        return rdma(
            osend.at[pl.ds(0, 3)], orecv.at[pl.ds(0, 3)], ox_s.at[0], ox_r.at[0], partner
        )

    def s_x(d):
        return rdma(
            stat.at[wrap(x + d, X)], srecv.at[x], sx_s.at[0], sx_r.at[0], xdev[d]
        )

    def s_all():
        return rdma(
            stat.at[pl.ds(0, 3)], srecv.at[pl.ds(0, 3)], sx_s.at[0], sx_r.at[0], partner
        )

    def a_y(d):
        return same(att.at[y], ay_s.at[0], ay_r.at[0], ydev[d])

    def a_all():
        return same(att.at[pl.ds(0, 3)], ay_s.at[0], ay_r.at[0], partner)

    def r_half(k, n):
        return rdma(
            pb.at[n, wrap(y + 2, Y), :, pl.ds(k * 256, 256)],
            rh.at[k, n],
            rh_s.at[k],
            rh_r.at[k, n],
            ynear[k],
        )

    def r_half_all(k):
        return same(rh.at[k], rh_s.at[k], rh_r.at[k, 0], ynear[k])

    def r_full(k, n):
        return rdma(
            pb.at[n, wrap(y + 1 - 2 * k, Y)],
            rb.at[k, n],
            rs_s.at[k],
            rs_r.at[k, n],
            ynear[k],
        )

    def r_full_all(k):
        return same(rb.at[k], rs_s.at[k], rs_r.at[k, 0], ynear[k])

    for cp in locals_[0:4]:
        cp.wait()
    pl.semaphore_wait(barrier, 9)

    lat_ring(0, 1, z)
    lat_ring(1, 1, z)
    lat_part(0, 0, z).start()
    for d in (1, 3, 2):
        q_x(d).start()
    for cp in locals_[4:9]:
        cp.wait()
    for way in (0, 1):
        dn_ring(way, 1, z).start()
    up_start(0)
    for d in (1, 3, 2):
        up_x(d).start()
    for k in (0, 1):
        dn_near(k, 0, z).start()
        st_near(k, 0).start()

    kta[...] = jnp.zeros_like(kta)
    ktb[...] = jnp.zeros_like(ktb)
    oacc[...] = jnp.zeros_like(oacc)
    for j in range(X):
        stat[j] = jnp.zeros((8, TOK), F32)
        stat[j, 0:1] = jnp.full((1, TOK), -jnp.inf, F32)
        stat[j, 2:3] = jnp.full((1, TOK), -jnp.inf, F32)
    for cp in locals_[9:]:
        cp.wait()
    wt[NOPE_A : NOPE_A + NOPE_B] = wkb0[...].T
    wt[NOPE_A + NOPE_B + V_A :] = wvb0[...].T
    kgain[0:DEPTH_A] = jnp.broadcast_to(gaina0[...], (TOK, DEPTH_A)).T
    kgain[DEPTH_A : DEPTH_A + DEPTH_B] = jnp.broadcast_to(gainb0[...], (TOK, DEPTH_B)).T
    pair = lax.broadcasted_iota(jnp.int32, (ROPE // 2, TOK), 0).astype(F32)
    freqs = jnp.exp(pair * (-math.log(THETA) / (ROPE // 2)))
    within = lax.broadcasted_iota(jnp.int32, (ROPE // 2, TOK), 1)

    def angles(i, carry):
        chunk = lax.div(i, 2) * 8 + x * 2 + lax.rem(i, 2)
        angle = (within + chunk * TOK).astype(F32) * freqs
        trig[i, 0 : ROPE // 2] = jnp.cos(angle)
        trig[i, ROPE // 2 : ROPE] = jnp.sin(angle)
        return carry

    lax.fori_loop(0, Z * C, angles, 0)

    def prep(zi, ci, i):
        rows = pl.ds(i * TOK, TOK)
        raw = lat[zi, ci, pl.ds(0, TOK), :].astype(F32)
        mean = jnp.mean(raw * raw, axis=-1, keepdims=True)
        nl = (raw * lax.rsqrt(mean + EPSILON) * lgain[...]).astype(BF16)
        kv = mm(wt[...], nl, NT).astype(BF16)
        vna[:, rows] = kv[NOPE_A + NOPE_B : NOPE_A + NOPE_B + V_A]
        vnb[:, rows] = kv[NOPE_A + NOPE_B + V_A :]
        rope = lat[zi, ci, pl.ds(TOK, ROPE), :].astype(F32)
        slot = zi * 2 + ci
        cosine = trig[slot, 0:16]
        sine = trig[slot, 16:32]
        square = jnp.sum(rope * rope, axis=0, keepdims=True)

        def one_head(nope, depth, base, dst):
            width = depth - ROPE
            wide = nope.astype(F32)
            total = jnp.sum(wide * wide, axis=0, keepdims=True) + square
            r = lax.rsqrt(total * (1.0 / depth) + EPSILON)
            dst[pl.ds(base, width), :] = (
                wide * r * kgain[pl.ds(base, width), :]
            ).astype(BF16)
            tail = rope * r * kgain[pl.ds(base + width, ROPE), :]
            first = tail[0:16]
            second = tail[16:32]
            dst[pl.ds(base + width, 16), :] = (first * cosine - second * sine).astype(BF16)
            dst[pl.ds(base + width + 16, 16), :] = (
                second * cosine + first * sine
            ).astype(BF16)

        one_head(kv[0:NOPE_A], DEPTH_A, 0, kta)
        one_head(kv[NOPE_A : NOPE_A + NOPE_B], DEPTH_B, DEPTH_A, ktb)
        ka[rows, :] = kta[...].T
        kb[rows, :] = ktb[...].T

    def prep_unit(t):
        odd = lax.rem(t, 2)
        s = lax.div(t + 1, 2)
        edge = lax.div(t, 7) + lax.div(7 - t, 7)
        flip_a = (1 - odd) * (1 - edge)
        flip_b = 1 - odd * (1 - edge)
        prep(wrap(z - s, Z), c + flip_a * (1 - 2 * c), 0)
        prep(wrap(z + s - 2 * s * edge, Z), c + flip_b * (1 - 2 * c), 1)

    peaks = {}

    def score(i, j):
        held = (s0, s1)[i % 2]
        for h, keys in enumerate((ka, kb)):
            top = None
            for lo in range(0, 2 * TOK, TOK):
                block = mm(keys[lo : lo + TOK], qt[j], NN)
                held[h * 2 * TOK + lo : h * 2 * TOK + lo + TOK] = block
                peak = jnp.max(block, axis=0, keepdims=True)
                top = peak if top is None else jnp.maximum(top, peak)
            peaks[i, h] = top

    def weigh(i, j):
        held = (s0, s1)[i % 2]
        for h, (values, scale, lo, width) in enumerate(
            ((va, SCALE_A, 0, V_A), (vb, SCALE_B, V_A, V_B))
        ):
            row = 2 * h
            old = stat[j, row : row + 1]
            new = jnp.maximum(old, peaks[i, h] * scale)
            factor = jnp.exp2(old - new)
            shifted = jnp.exp2(held[h * 2 * TOK : (h + 1) * 2 * TOK] * scale - new)
            stat[j, row : row + 1] = new
            stat[j, row + 1 : row + 2] = stat[j, row + 1 : row + 2] * factor + jnp.sum(
                shifted, axis=0, keepdims=True
            )
            part = mm(values[...], shifted.astype(BF16), NN)
            oacc[j, lo : lo + width] = oacc[j, lo : lo + width] * factor + part

    def attend(order, between, done):
        score(0, order[0])
        for i in range(X):
            if i + 1 < X:
                score(i + 1, order[i + 1])
            if i + 2 == X:
                between()
            weigh(i, order[i])
            done(i)

    def first_unit():
        for d in (0, 1, 3, 2):
            if d == 1:
                lat_step(1)
            elif d == 3:
                lat_step(2)
            elif d == 2:
                dn_step(1)
                up_step(0, 1)
            if d:
                q_wait(d)
            j = wrap(x - d, X)
            score(0, j)
            weigh(0, j)
        lat_spread(1)
        prep_unit(jnp.int32(1))

    def last_unit():
        steps = (2, 1, 3, 0)

        def done(i):
            d = steps[i]
            j = wrap(x + d, X)
            target, slot = (osend, j) if d else (orecv, x)
            inverse = 1.0 / stat[j]
            target[slot, 0:V_A] = (oacc[j, 0:V_A] * inverse[1:2]).astype(BF16)
            target[slot, V_A:OUT] = (oacc[j, V_A:OUT] * inverse[3:4]).astype(BF16)
            if d:
                s_x(d).start()
                o_x(d).start()
            else:
                srecv[x] = stat[x]

        attend([wrap(x + d, X) for d in steps], lambda: None, done)

    def lat_step(s):
        zm = wrap(z - s, Z)
        zp = wrap(z + s, Z)
        lat_ring_wait(0, s)
        if s < 4:
            lat_ring(0, s + 1, zm)
            lat_ring_wait(1, s)
            if s < 3:
                lat_ring(1, s + 1, zp)
            lat_y(1, s, zp)
        lat_y(0, s, zm)

    def lat_spread(s):
        lat_y_wait(0, s)
        lat_part(0, s, wrap(z - s, Z)).start()
        if s < 4:
            lat_y_wait(1, s)
            lat_part(1, s, wrap(z + s, Z)).start()

    def dn_step(s):
        zm = wrap(z - s, Z)
        zp = wrap(z + s, Z)
        bulk = s // 3
        dn_ring(0, s, zm).wait_recv()
        if s < 4:
            dn_ring(0, s + 1, zm).start()
            dn_ring(1, s, zp).wait_recv()
            if s < 3:
                dn_ring(1, s + 1, zp).start()
        for k in (0, 1):
            dn_near(k, bulk, zm).start()
            if s < 4:
                dn_near(k, bulk, zp).start()

    def dn_forward(bulk):
        for k in (0, 1):
            dn_near_wait(k, bulk)
            for s in ((0, 1, 2), (3, 4))[bulk]:
                dn_relay(k, wrap(z - s, Z)).start()
                if 0 < s < 4:
                    dn_relay(k, wrap(z + s, Z)).start()

    def part_wait(s):
        lat_part(0, s, z).wait_recv()
        if 0 < s < 4:
            lat_part(1, s, z).wait_recv()

    def before(t):
        if t == 1:
            lat_step(3)
        elif t == 2:
            lat_spread(2)
            part_wait(1)
            prep_unit(jnp.int32(2))
        elif t == 3:
            part_wait(2)
        elif t == 4:
            lat_spread(3)
        elif t == 5:
            lat_spread(4)
            part_wait(3)
        elif t == 6:
            part_wait(4)

    def after(t):
        if t == 0:
            for k in (0, 1):
                st_near(k, 1).start()
        elif t == 1:
            dn_step(2)
            up_step(0, 2)
            up_x_all().wait_recv()
            up_start(1)
            up_start(2)
        elif t == 2:
            lat_step(4)
            for k in (0, 1):
                wo_near(k, 0).start()
        elif t == 3:
            dn_step(3)
            up_step(0, 3)
            for k in (0, 1):
                wo_near(k, 1).start()
        elif t == 4:
            up_step(1, 1)
            for k in (0, 1):
                st_near(k, 0).wait_recv()
                st_relay(k).start()
            dn_forward(0)
        elif t == 5:
            up_step(2, 1)
            dn_step(4)
            up_step(0, 4)
        elif t == 6:
            up_step(1, 2)
            for k in (0, 1):
                wo_near(k, 0).wait_recv()
                wo_relay(k).start()
        elif t == 7:
            up_step(2, 2)
            for k in (0, 1):
                wo_near(k, 1).wait_recv()
                wo_part(1 + 2 * k).start()

    def at(t, fn, times):
        for i in times:
            pl.when(t == i)(functools.partial(fn, i))

    def unit(t, carry):
        at(t, before, range(1, 7))
        va[...] = vna[...]
        vb[...] = vnb[...]
        @pl.when(t == 0)
        def _():
            first_unit()

        @pl.when(t == 1)
        def _():
            attend(range(X), lambda: None, lambda i: None)

        @pl.when((t > 1) & (t < 7))
        def _():
            attend(range(X), lambda: prep_unit(t + 1), lambda i: None)

        @pl.when(t == 7)
        def _():
            last_unit()

        at(t, after, range(8))
        return carry

    part_wait(0)
    prep_unit(jnp.int32(0))
    lax.fori_loop(0, 8, unit, 0)

    dn_forward(1)
    for d in (0, 1, 3):
        dn_part(d).start()
    up_step(1, 3)
    s_all().wait_recv()
    o_all().wait_recv()

    for row, lo, width in ((0, 0, V_A), (2, V_A, V_B)):
        peaks = [srecv[i, row : row + 1] for i in range(X)]
        top = functools.reduce(jnp.maximum, peaks)
        shares = [srecv[i, row + 1 : row + 2] * jnp.exp2(peaks[i] - top) for i in range(X)]
        inverse = 1.0 / (shares[0] + shares[1] + shares[2] + shares[3])
        mixed = orecv[0, lo : lo + width].astype(F32) * (shares[0] * inverse)
        for i in range(1, X):
            mixed = mixed + orecv[i, lo : lo + width].astype(F32) * (shares[i] * inverse)
        att[y, pl.ds(lo, width), :] = mixed.astype(BF16)
    for d in (2, 1, 3):
        a_y(d).start()

    up_step(2, 3)
    up_step(1, 4)
    wo_relay_all().wait_recv()
    wo_part(2).start()
    dn_relay_all().wait_recv()
    dn_part(2).start()
    for k in (0, 1):
        st_near(k, 1).wait_recv()
    st_relay_all().wait_recv()
    wo_part_all().wait_recv()
    up_step(2, 4)
    a_all().wait_recv()

    attended = att[...].reshape(Y * OUT, TOK).T
    squares = jnp.zeros((TOK, 1), F32)
    for n in range(4):
        cols = slice(n * 512, n * 512 + 512)
        weights = wo[:, :, cols].reshape(Y * OUT, 512)
        mixed = mm(attended, weights, NN)
        summed = (st[:, :, cols].reshape(TOK, 512).astype(F32) + mixed).astype(BF16)
        res[:, cols] = summed
        wide = summed.astype(F32)
        squares = squares + jnp.sum(wide * wide, axis=-1, keepdims=True)
    r = lax.rsqrt(squares * (1.0 / D) + EPSILON)
    for n in range(4):
        cols = slice(n * 512, n * 512 + 512)
        nrm[:, cols] = (res[:, cols].astype(F32) * r * ngain[:, cols]).astype(BF16)

    up_part_all().wait_recv()
    for n in range(4):
        cols = slice(n * 256, n * 256 + 256)
        hidden = jnp.maximum(mm(nrm[...], up[:, :, :, :, cols].reshape(D, 256), NN), 0.0)
        act[:, cols] = (hidden * hidden).astype(BF16)

    dn_part_all().wait_recv()

    for n in range(4):
        weights = dn[2 * n : 2 * n + 2].reshape(512, FF)
        part = mm(act[...], weights, NT).astype(BF16)
        pb[n] = part.reshape(Y, OWN, 512)
        for k in (0, 1):
            r_half(k, n).start()

    for n in range(4):
        for k in (0, 1):
            r_half(k, n).wait_recv()
            dest = wrap(y + 1 - 2 * k, Y)
            cols = slice(k * 256, k * 256 + 256)
            pb[n, dest, :, cols] = (
                pb[n, dest, :, cols].astype(F32) + rh[k, n].astype(F32)
            ).astype(BF16)
            r_full(k, n).start()
    stores = [
        pltpu.make_async_copy(ob.at[n], out.at[:, pl.ds(n * 512, 512)], loc.at[n])
        for n in range(4)
    ]
    for n in range(4):
        cols = slice(n * 512, n * 512 + 512)
        total = pb[n, y].astype(F32)
        for k in (0, 1):
            r_full(k, n).wait_recv()
            total = total + rb[k, n].astype(F32)
        ob[n] = (res[mine, cols].astype(F32) + total).astype(BF16)
        if n:
            stores[n - 1].start()
    stores[3].start()

    same(lat.at[pl.ds(0, 7), c, pl.ds(0, OWN + ROPE)], lat_s.at[0], lat_r.at[0, 0], partner).wait_send()
    same(
        lat.at[pl.ds(0, 7), c, pl.ds(0, 3 * OWN)], laty_s.at[0], laty_r.at[0, 0], partner
    ).wait_send()
    same(lat.at[:, c], latp_s.at[0], latp_r.at[0, 0], partner).wait_send()
    same(dn.at[pl.ds(0, 7), x, c], dnz_s.at[0], dnz_r.at[0, 0], partner).wait_send()
    same(st.at[pl.ds(0, 2)], st_s.at[0], st_r.at[0], partner).wait_send()
    same(wo.at[pl.ds(0, 2), :, half], wo_s.at[0], wo_r.at[0], partner).wait_send()
    q_all().wait_send()
    up_x_all().wait_send()
    up_ring_all().wait_send()
    up_part_all().wait_send()
    same(dn.at[:, pl.ds(0, 2), c], dnx_s.at[0], dnx_r.at[0, 0], partner).wait_send()
    dn_relay_all().wait_send()
    dn_part_all().wait_send()
    st_relay_all().wait_send()
    wo_relay_all().wait_send()
    wo_part_all().wait_send()
    o_all().wait_send()
    s_all().wait_send()
    a_all().wait_send()
    for k in (0, 1):
        r_half_all(k).wait_send()
        r_full_all(k).wait_send()
    for cp in stores:
        cp.wait()


def body(
    stream,
    query_a,
    query_b,
    latent,
    rotary_key,
    latent_gain,
    key_gain_a,
    key_gain_b,
    w_key_a,
    w_value_a,
    w_key_b,
    w_value_b,
    w_out_a,
    w_out_b,
    norm_gain,
    w_up,
    w_down,
):
    hbm = pl.BlockSpec(memory_space=pltpu.HBM)
    dma = pltpu.SemaphoreType.DMA
    return pl.pallas_call(
        kernel,
        out_shape=jax.ShapeDtypeStruct((OWN, D), BF16),
        in_specs=[hbm] * 17,
        out_specs=hbm,
        scratch_shapes=[
            pltpu.VMEM((RANK, NOPE_B), BF16),
            pltpu.VMEM((RANK, V_B), BF16),
            pltpu.VMEM((1, RANK), F32),
            pltpu.VMEM((1, DEPTH_A), F32),
            pltpu.VMEM((1, DEPTH_B), F32),
            pltpu.VMEM((1, D), F32),
            pltpu.VMEM((KV, RANK), BF16),
            pltpu.VMEM((DEPTH_A + DEPTH_B, TOK), F32),
            pltpu.VMEM((Z * C, ROPE, TOK), F32),
            pltpu.VMEM((4 * TOK, TOK), F32),
            pltpu.VMEM((4 * TOK, TOK), F32),
            pltpu.VMEM((Z, C, TOK + ROPE, RANK), BF16),
            pltpu.VMEM((X, TOK, DEPTH_A + DEPTH_B), BF16),
            pltpu.VMEM((Z, X, C, 32, FF), BF16),
            pltpu.VMEM((Z, X, C, 32, FF), BF16),
            pltpu.VMEM((Y, OUT, D), BF16),
            pltpu.VMEM((Y, OWN, D), BF16),
            pltpu.VMEM((256, TOK), BF16),
            pltpu.VMEM((256, TOK), BF16),
            pltpu.VMEM((2 * TOK, 256), BF16),
            pltpu.VMEM((2 * TOK, 256), BF16),
            pltpu.VMEM((V_A, 2 * TOK), BF16),
            pltpu.VMEM((V_B, 2 * TOK), BF16),
            pltpu.VMEM((V_A, 2 * TOK), BF16),
            pltpu.VMEM((V_B, 2 * TOK), BF16),
            pltpu.VMEM((X, OUT, TOK), F32),
            pltpu.VMEM((X, 8, TOK), F32),
            pltpu.VMEM((X, OUT, TOK), BF16),
            pltpu.VMEM((X, OUT, TOK), BF16),
            pltpu.VMEM((X, 8, TOK), F32),
            pltpu.VMEM((Y, OUT, TOK), BF16),
            pltpu.VMEM((TOK, D), BF16),
            pltpu.VMEM((TOK, D), BF16),
            pltpu.VMEM((TOK, FF), BF16),
            pltpu.VMEM((4, Y, OWN, 512), BF16),
            pltpu.VMEM((2, 4, OWN, 512), BF16),
            pltpu.VMEM((2, 4, OWN, 256), BF16),
            pltpu.VMEM((4, OWN, 512), BF16),
            dma((17,)),
            dma((1,)),
            dma((2, 5)),
            dma((1,)),
            dma((2, 5)),
            dma((1,)),
            dma((2, 5)),
            dma((1,)),
            dma((3,)),
            dma((1,)),
            dma((1,)),
            dma((1,)),
            dma((2, 3, 5)),
            dma((1,)),
            dma((1,)),
            dma((1,)),
            dma((2, 5)),
            dma((2,)),
            dma((2, 2)),
            dma((1,)),
            dma((1,)),
            dma((1,)),
            dma((2,)),
            dma((2, 2)),
            dma((1,)),
            dma((2,)),
            dma((2, 2)),
            dma((1,)),
            dma((1,)),
            dma((1,)),
            dma((1,)),
            dma((1,)),
            dma((1,)),
            dma((1,)),
            dma((1,)),
            dma((1,)),
            dma((2,)),
            dma((2, 4)),
            dma((2,)),
            dma((2, 4)),
        ],
        compiler_params=pltpu.CompilerParams(
            collective_id=0, has_side_effects=True, vmem_limit_bytes=60 * 1024 * 1024,
        ),
        name="layer",
    )(
        latent,
        rotary_key.T,
        query_a.T,
        query_b.T,
        w_up,
        w_down.T,
        w_out_a,
        w_out_b,
        stream,
        w_key_a.T,
        w_key_b,
        w_value_a.T,
        w_value_b,
        latent_gain.reshape(1, RANK),
        key_gain_a.reshape(1, DEPTH_A),
        key_gain_b.reshape(1, DEPTH_B),
        norm_gain.reshape(1, D),
    )


def solution(mesh):
    in_specs = (
        P(("sp", "tp"), None),
        P("sp", "tp"),
        P("sp", "tp"),
        P("sp", None),
        P("sp", None),
        P(),
        P(),
        P(),
        P(None, "tp"),
        P(None, "tp"),
        P(None, "tp"),
        P(None, "tp"),
        P("tp", None),
        P("tp", None),
        P(),
        P("sp", "tp"),
        P("tp", "sp"),
    )
    out_specs = P(("sp", "tp"), None)
    return jax.shard_map(body, mesh=mesh, in_specs=in_specs, out_specs=out_specs, check_vma=False)
```

```python
import functools
import math

import jax
import jax.numpy as jnp
from jax import lax
from jax.experimental import pallas as pl
from jax.experimental.pallas import tpu as pltpu
from jax.sharding import PartitionSpec as P

NOPE_A = 64
V_A = 64
NOPE_B = 128
V_B = 128
ROPE = 32
DEPTH_A = NOPE_A + ROPE
DEPTH_B = NOPE_B + ROPE
KV = NOPE_A + NOPE_B + V_A + V_B
OUT = V_A + V_B
RANK = 256
D = 2048
FF = 1024
TOK = 256
OWN = 64
Z, X, C, Y = 8, 4, 2, 4
SETS = ((0,), (1, 3), (2,))
EPSILON = 1e-06
THETA = 10000.0
LOG2E = 1.4426950408889634
SCALE_A = DEPTH_A ** (-0.5) * LOG2E
SCALE_B = DEPTH_B ** (-0.5) * LOG2E
NT = (((1,), (1,)), ((), ()))
NN = (((1,), (0,)), ((), ()))
F32 = jnp.float32
BF16 = jnp.bfloat16


def mm(a, b, dims):
    return lax.dot_general(a, b, dims, preferred_element_type=F32)


def kernel(
    lat_in,
    rope_in,
    qa_in,
    qb_in,
    up_in,
    dn_in,
    woa_in,
    wob_in,
    st_in,
    wka_in,
    wkb_in,
    wva_in,
    wvb_in,
    lgain_in,
    gaina_in,
    gainb_in,
    ngain_in,
    out,
    wkb0,
    wvb0,
    lgain,
    gaina0,
    gainb0,
    ngain,
    wt,
    kgain,
    trig,
    s0,
    s1,
    lat,
    qt,
    up,
    dn,
    wo,
    st,
    kta,
    ktb,
    ka,
    kb,
    va,
    vb,
    vna,
    vnb,
    oacc,
    stat,
    osend,
    orecv,
    srecv,
    att,
    res,
    nrm,
    act,
    pb,
    rb,
    rh,
    ob,
    loc,
    lat_s,
    lat_r,
    laty_s,
    laty_r,
    latp_s,
    latp_r,
    q_s,
    q_r,
    upx_s,
    upx_r,
    upz_s,
    upz_r,
    upp_s,
    upp_r,
    dnz_s,
    dnz_r,
    dnx_s,
    dnx_r,
    dnr_r,
    dnp_s,
    dnp_r,
    st_s,
    st_r,
    str_r,
    wo_s,
    wo_r,
    wor_r,
    wop_s,
    wop_r,
    ox_s,
    ox_r,
    sx_s,
    sx_r,
    ay_s,
    ay_r,
    rh_s,
    rh_r,
    rs_s,
    rs_r,
):
    sp = lax.axis_index("sp")
    y = lax.axis_index("tp")
    z = lax.div(sp, 8)
    x = lax.rem(lax.div(sp, 2), 4)
    c = lax.rem(sp, 2)
    oc = 1 - c

    def wrap(v, n):
        return lax.rem(v + 2 * n, n)

    def dev(z_, x_, c_, y_):
        return {"sp": z_ * 8 + x_ * 2 + c_, "tp": y_}

    partner = dev(z, x, oc, y)
    zdev = (dev(wrap(z + 1, Z), x, c, y), dev(wrap(z - 1, Z), x, c, y))
    xdev = [None] + [dev(z, wrap(x + d, X), c, y) for d in (1, 2, 3)]
    xnear = (dev(z, wrap(x + 1, X), c, y), dev(z, wrap(x - 1, X), c, y))
    ynear = (dev(z, x, c, wrap(y + 1, Y)), dev(z, x, c, wrap(y - 1, Y)))
    ydev = [None] + [dev(z, x, c, wrap(y + d, Y)) for d in (1, 2, 3)]

    def rdma(src, dst, ss, rs, where):
        return pltpu.make_async_remote_copy(
            src_ref=src,
            dst_ref=dst,
            send_sem=ss,
            recv_sem=rs,
            device_id=where,
            device_id_type=pl.DeviceIdType.MESH,
        )

    def same(ref, ss, rs, where):
        return rdma(ref, ref, ss, rs, where)

    pairs = (
        (lat_in, lat.at[z, c, pl.ds(0, TOK)]),
        (rope_in, lat.at[z, c, pl.ds(TOK, ROPE)]),
        (qa_in, qt.at[x, pl.ds(0, DEPTH_A)]),
        (qb_in, qt.at[x, pl.ds(DEPTH_A, DEPTH_B)]),
        (dn_in, dn.at[z, x, c]),
        (up_in, up.at[z, x, c]),
        (st_in, st.at[y]),
        (woa_in, wo.at[y, pl.ds(0, V_A)]),
        (wob_in, wo.at[y, pl.ds(V_A, V_B)]),
        (wka_in, wt.at[pl.ds(0, NOPE_A)]),
        (wva_in, wt.at[pl.ds(NOPE_A + NOPE_B, V_A)]),
        (wkb_in, wkb0),
        (wvb_in, wvb0),
        (lgain_in, lgain),
        (gaina_in, gaina0),
        (gainb_in, gainb0),
        (ngain_in, ngain),
    )
    locals_ = [
        pltpu.make_async_copy(src, dst, loc.at[i]) for i, (src, dst) in enumerate(pairs)
    ]
    for cp in locals_:
        cp.start()

    barrier = pltpu.get_barrier_semaphore()
    for where in [partner, *zdev, *xdev[1:], *ydev[1:]]:
        pl.semaphore_signal(
            barrier, inc=1, device_id=where, device_id_type=pl.DeviceIdType.MESH
        )

    mine = pl.ds(pl.multiple_of(y * OWN, OWN), OWN)

    def lat_ring(way, s, zsrc):
        for rows in (mine, pl.ds(TOK, ROPE)):
            same(lat.at[zsrc, c, rows], lat_s.at[0], lat_r.at[s - 1 + 4 * way], zdev[way]).start()

    def lat_ring_wait(way, s):
        ref = lat.at[z, c, pl.ds(0, OWN + ROPE)]
        same(ref, lat_s.at[0], lat_r.at[s - 1 + 4 * way], zdev[way]).wait_recv()

    def lat_y(way, s, zsrc):
        for d in (1, 3, 2):
            same(lat.at[zsrc, c, mine], laty_s.at[0], laty_r.at[s - 1 + 4 * way], ydev[d]).start()

    def lat_y_wait(way, s):
        ref = lat.at[z, c, pl.ds(0, 3 * OWN)]
        same(ref, laty_s.at[0], laty_r.at[s - 1 + 4 * way], partner).wait_recv()

    def lat_part(way, s, zsrc):
        return same(lat.at[zsrc, c], latp_s.at[0], latp_r.at[s + 4 * way], partner)

    def q_x(d):
        return same(qt.at[x], q_s.at[0], q_r.at[d - 1], xdev[d])

    def q_all():
        return same(qt.at[pl.ds(0, 3)], q_s.at[0], q_r.at[0], partner)

    def q_wait(d):
        q_x(d).wait_recv()

    def up_x(d):
        return same(up.at[z, x, c], upx_s.at[0], upx_r.at[0], xdev[d])

    def up_x_all():
        return same(up.at[z, pl.ds(0, 3), c], upx_s.at[0], upx_r.at[0], partner)

    def up_hop(way, g, s, zsrc):
        for d in SETS[g]:
            ref = up.at[zsrc, wrap(x - d, X), c]
            same(ref, upz_s.at[0], upz_r.at[g, s - 1 + 4 * (1 - way)], zdev[way]).start()

    def up_hop_wait(way, g, s):
        ref = up.at[z, pl.ds(0, len(SETS[g])), c]
        same(ref, upz_s.at[0], upz_r.at[g, s - 1 + 4 * (1 - way)], zdev[way]).wait_recv()

    def up_ring_all():
        ref = up.at[pl.ds(0, 7), :, c]
        return same(ref, upz_s.at[0], upz_r.at[0, 0], partner)

    def up_part(g, zsrc):
        for d in SETS[g]:
            ref = up.at[zsrc, wrap(x - d, X), c]
            same(ref, upp_s.at[0], upp_r.at[0], partner).start()

    def up_part_all():
        return same(up.at[:, :, c], upp_s.at[0], upp_r.at[0], partner)

    def up_start(g):
        up_hop(0, g, 1, z)
        up_hop(1, g, 1, z)
        up_part(g, z)

    def up_step(g, s):
        um = wrap(z - s, Z)
        un = wrap(z + s, Z)
        up_hop_wait(1, g, s)
        if s < 4:
            up_hop(1, g, s + 1, un)
        up_part(g, un)
        if s < 4:
            up_hop_wait(0, g, s)
            if s < 3:
                up_hop(0, g, s + 1, um)
            up_part(g, um)

    def dn_ring(way, s, zsrc):
        return same(dn.at[zsrc, x, c], dnz_s.at[0], dnz_r.at[s - 1 + 4 * way], zdev[way])

    def dn_near(k, b, zsrc):
        return same(dn.at[zsrc, x, c], dnx_s.at[0], dnx_r.at[k, b], xnear[k])

    def dn_near_wait(k, b):
        ref = dn.at[pl.ds(0, 5 - 2 * b), wrap(x - 1 + 2 * k, X), c]
        same(ref, dnx_s.at[0], dnx_r.at[k, b], xnear[k]).wait_recv()

    def dn_relay(k, zsrc):
        ref = dn.at[zsrc, wrap(x - 1 + 2 * k, X), c, pl.ds(16 * k, 16)]
        return same(ref, dnx_s.at[1], dnr_r.at[0], xnear[k])

    def dn_relay_all():
        return same(dn.at[:, x, c], dnx_s.at[1], dnr_r.at[0], partner)

    def dn_part(d):
        return same(dn.at[:, wrap(x - d, X), c], dnp_s.at[0], dnp_r.at[0], partner)

    def dn_part_all():
        return same(dn.at[:, :, c], dnp_s.at[0], dnp_r.at[0], partner)

    def st_near(k, i):
        rows = pl.ds((OWN // 2) * (k if i == 0 else 1 - k), OWN // 2)
        return same(st.at[y, rows], st_s.at[0], st_r.at[k, i], ynear[k])

    def st_relay(k):
        ref = st.at[wrap(y - 1 + 2 * k, Y), pl.ds(k * (OWN // 2), OWN // 2)]
        return same(ref, st_s.at[1], str_r.at[0], ynear[k])

    def st_relay_all():
        return same(st.at[y], st_s.at[1], str_r.at[0], ynear[0])

    half = pl.ds(pl.multiple_of(c * (D // 2), D // 2), D // 2)

    def wo_cols(k):
        return pl.ds(pl.multiple_of(c * (D // 2) + k * (D // 4), D // 4), D // 4)

    def wo_near(k, i):
        cols = wo_cols(k if i == 0 else 1 - k)
        return same(wo.at[y, :, cols], wo_s.at[0], wo_r.at[k, i], ynear[k])

    def wo_relay(k):
        ref = wo.at[wrap(y - 1 + 2 * k, Y), :, wo_cols(k)]
        return same(ref, wo_s.at[1], wor_r.at[0], ynear[k])

    def wo_relay_all():
        return same(wo.at[y, :, half], wo_s.at[1], wor_r.at[0], ynear[0])

    def wo_part(d):
        return same(wo.at[wrap(y - d, Y), :, half], wop_s.at[0], wop_r.at[0], partner)

    def wo_part_all():
        return same(wo.at[pl.ds(0, 3), :, half], wop_s.at[0], wop_r.at[0], partner)

    def lanes(e):
        return pl.ds(e * (TOK // 2), TOK // 2)

    def o_x(d, e):
        return rdma(
            osend.at[wrap(x + d, X), :, lanes(e)],
            orecv.at[x, :, lanes(e)],
            ox_s.at[0],
            ox_r.at[e],
            xdev[d],
        )

    def o_wait(e):
        ref = orecv.at[pl.ds(0, 3), :, lanes(e)]
        rdma(ref, ref, ox_s.at[0], ox_r.at[e], partner).wait_recv()

    def o_all():
        return rdma(
            osend.at[pl.ds(0, 3)], orecv.at[pl.ds(0, 3)], ox_s.at[0], ox_r.at[0], partner
        )

    def s_x(d):
        return rdma(
            stat.at[wrap(x + d, X)], srecv.at[x], sx_s.at[0], sx_r.at[0], xdev[d]
        )

    def s_all():
        return rdma(
            stat.at[pl.ds(0, 3)], srecv.at[pl.ds(0, 3)], sx_s.at[0], sx_r.at[0], partner
        )

    def a_y(d, e):
        return same(att.at[y, :, lanes(e)], ay_s.at[0], ay_r.at[e], ydev[d])

    def a_wait(e):
        ref = att.at[pl.ds(0, 3), :, lanes(e)]
        same(ref, ay_s.at[0], ay_r.at[e], partner).wait_recv()

    def a_all():
        return same(att.at[pl.ds(0, 3)], ay_s.at[0], ay_r.at[0], partner)

    def r_half(k, n):
        return rdma(
            pb.at[n, wrap(y + 2, Y), :, pl.ds(k * 256, 256)],
            rh.at[k, n],
            rh_s.at[k],
            rh_r.at[k, n],
            ynear[k],
        )

    def r_half_all(k):
        return same(rh.at[k], rh_s.at[k], rh_r.at[k, 0], ynear[k])

    def r_full(k, n):
        return rdma(
            pb.at[n, wrap(y + 1 - 2 * k, Y)],
            rb.at[k, n],
            rs_s.at[k],
            rs_r.at[n],
            ynear[k],
        )

    def r_full_all(k):
        return same(rb.at[k], rs_s.at[k], rs_r.at[0], ynear[k])

    def r_full_wait(n):
        same(rb.at[:, n], rs_s.at[0], rs_r.at[n], ynear[0]).wait_recv()

    for cp in locals_[0:4]:
        cp.wait()
    pl.semaphore_wait(barrier, 9)

    lat_ring(0, 1, z)
    lat_ring(1, 1, z)
    lat_part(0, 0, z).start()
    for d in (1, 3, 2):
        q_x(d).start()
    for cp in locals_[4:9]:
        cp.wait()
    for way in (0, 1):
        dn_ring(way, 1, z).start()
    up_start(0)
    for d in (1, 3, 2):
        up_x(d).start()
    for k in (0, 1):
        dn_near(k, 0, z).start()
        st_near(k, 0).start()

    kta[...] = jnp.zeros_like(kta)
    ktb[...] = jnp.zeros_like(ktb)
    oacc[...] = jnp.zeros_like(oacc)
    for j in range(X):
        stat[j] = jnp.zeros((8, TOK), F32)
        stat[j, 0:1] = jnp.full((1, TOK), -jnp.inf, F32)
        stat[j, 2:3] = jnp.full((1, TOK), -jnp.inf, F32)
    for cp in locals_[9:]:
        cp.wait()
    wt[NOPE_A : NOPE_A + NOPE_B] = wkb0[...].T
    wt[NOPE_A + NOPE_B + V_A :] = wvb0[...].T
    kgain[0:DEPTH_A] = jnp.broadcast_to(gaina0[...], (TOK, DEPTH_A)).T
    kgain[DEPTH_A : DEPTH_A + DEPTH_B] = jnp.broadcast_to(gainb0[...], (TOK, DEPTH_B)).T
    pair = lax.broadcasted_iota(jnp.int32, (ROPE // 2, TOK), 0).astype(F32)
    freqs = jnp.exp(pair * (-math.log(THETA) / (ROPE // 2)))
    within = lax.broadcasted_iota(jnp.int32, (ROPE // 2, TOK), 1)

    def angles(i, carry):
        chunk = lax.div(i, 2) * 8 + x * 2 + lax.rem(i, 2)
        angle = (within + chunk * TOK).astype(F32) * freqs
        trig[i, 0 : ROPE // 2] = jnp.cos(angle)
        trig[i, ROPE // 2 : ROPE] = jnp.sin(angle)
        return carry

    lax.fori_loop(0, Z * C, angles, 0)

    def prep(zi, ci, i):
        rows = pl.ds(i * TOK, TOK)
        raw = lat[zi, ci, pl.ds(0, TOK), :].astype(F32)
        mean = jnp.mean(raw * raw, axis=-1, keepdims=True)
        nl = (raw * lax.rsqrt(mean + EPSILON) * lgain[...]).astype(BF16)
        kv = mm(wt[...], nl, NT).astype(BF16)
        vna[:, rows] = kv[NOPE_A + NOPE_B : NOPE_A + NOPE_B + V_A]
        vnb[:, rows] = kv[NOPE_A + NOPE_B + V_A :]
        rope = lat[zi, ci, pl.ds(TOK, ROPE), :].astype(F32)
        slot = zi * 2 + ci
        cosine = trig[slot, 0:16]
        sine = trig[slot, 16:32]
        square = jnp.sum(rope * rope, axis=0, keepdims=True)

        def one_head(nope, depth, base, dst):
            width = depth - ROPE
            wide = nope.astype(F32)
            total = jnp.sum(wide * wide, axis=0, keepdims=True) + square
            r = lax.rsqrt(total * (1.0 / depth) + EPSILON)
            dst[pl.ds(base, width), :] = (
                wide * r * kgain[pl.ds(base, width), :]
            ).astype(BF16)
            tail = rope * r * kgain[pl.ds(base + width, ROPE), :]
            first = tail[0:16]
            second = tail[16:32]
            dst[pl.ds(base + width, 16), :] = (first * cosine - second * sine).astype(BF16)
            dst[pl.ds(base + width + 16, 16), :] = (
                second * cosine + first * sine
            ).astype(BF16)

        one_head(kv[0:NOPE_A], DEPTH_A, 0, kta)
        one_head(kv[NOPE_A : NOPE_A + NOPE_B], DEPTH_B, DEPTH_A, ktb)
        ka[rows, :] = kta[...].T
        kb[rows, :] = ktb[...].T

    def prep_unit(t):
        odd = lax.rem(t, 2)
        s = lax.div(t + 1, 2)
        edge = lax.div(t, 7) + lax.div(7 - t, 7)
        flip_a = (1 - odd) * (1 - edge)
        flip_b = 1 - odd * (1 - edge)
        prep(wrap(z - s, Z), c + flip_a * (1 - 2 * c), 0)
        prep(wrap(z + s - 2 * s * edge, Z), c + flip_b * (1 - 2 * c), 1)

    peaks = {}

    def score(i, j):
        held = (s0, s1)[i % 2]
        for h, keys in enumerate((ka, kb)):
            top = None
            for lo in range(0, 2 * TOK, TOK):
                block = mm(keys[lo : lo + TOK], qt[j], NN)
                held[h * 2 * TOK + lo : h * 2 * TOK + lo + TOK] = block
                peak = jnp.max(block, axis=0, keepdims=True)
                top = peak if top is None else jnp.maximum(top, peak)
            peaks[i, h] = top

    def weigh(i, j):
        held = (s0, s1)[i % 2]
        for h, (values, scale, lo, width) in enumerate(
            ((va, SCALE_A, 0, V_A), (vb, SCALE_B, V_A, V_B))
        ):
            row = 2 * h
            old = stat[j, row : row + 1]
            new = jnp.maximum(old, peaks[i, h] * scale)
            factor = jnp.exp2(old - new)
            shifted = jnp.exp2(held[h * 2 * TOK : (h + 1) * 2 * TOK] * scale - new)
            stat[j, row : row + 1] = new
            stat[j, row + 1 : row + 2] = stat[j, row + 1 : row + 2] * factor + jnp.sum(
                shifted, axis=0, keepdims=True
            )
            part = mm(values[...], shifted.astype(BF16), NN)
            oacc[j, lo : lo + width] = oacc[j, lo : lo + width] * factor + part

    def attend(order, between, done):
        score(0, order[0])
        for i in range(X):
            if i + 1 < X:
                score(i + 1, order[i + 1])
            if i + 2 == X:
                between()
            weigh(i, order[i])
            done(i)

    def first_unit():
        for d in (0, 1, 3, 2):
            if d == 1:
                lat_step(1)
            elif d == 3:
                lat_step(2)
            elif d == 2:
                dn_step(1)
                up_step(0, 1)
            if d:
                q_wait(d)
            j = wrap(x - d, X)
            score(0, j)
            weigh(0, j)
        lat_spread(1)
        prep_unit(jnp.int32(1))

    def last_unit():
        steps = (2, 1, 3, 0)

        def done(i):
            d = steps[i]
            j = wrap(x + d, X)
            target, slot = (osend, j) if d else (orecv, x)
            inverse = 1.0 / stat[j]
            target[slot, 0:V_A] = (oacc[j, 0:V_A] * inverse[1:2]).astype(BF16)
            target[slot, V_A:OUT] = (oacc[j, V_A:OUT] * inverse[3:4]).astype(BF16)
            if d:
                s_x(d).start()
                o_x(d, 0).start()
            else:
                srecv[x] = stat[x]

        attend([wrap(x + d, X) for d in steps], lambda: None, done)
        for d in (2, 1, 3):
            o_x(d, 1).start()

    def lat_step(s):
        zm = wrap(z - s, Z)
        zp = wrap(z + s, Z)
        lat_ring_wait(0, s)
        if s < 4:
            lat_ring(0, s + 1, zm)
            lat_ring_wait(1, s)
            if s < 3:
                lat_ring(1, s + 1, zp)
            lat_y(1, s, zp)
        lat_y(0, s, zm)

    def lat_spread(s):
        lat_y_wait(0, s)
        lat_part(0, s, wrap(z - s, Z)).start()
        if s < 4:
            lat_y_wait(1, s)
            lat_part(1, s, wrap(z + s, Z)).start()

    def dn_step(s):
        zm = wrap(z - s, Z)
        zp = wrap(z + s, Z)
        bulk = s // 3
        dn_ring(0, s, zm).wait_recv()
        if s < 4:
            dn_ring(0, s + 1, zm).start()
            dn_ring(1, s, zp).wait_recv()
            if s < 3:
                dn_ring(1, s + 1, zp).start()
        for k in (0, 1):
            dn_near(k, bulk, zm).start()
            if s < 4:
                dn_near(k, bulk, zp).start()

    def dn_forward(bulk):
        for k in (0, 1):
            dn_near_wait(k, bulk)
            for s in ((0, 1, 2), (3, 4))[bulk]:
                dn_relay(k, wrap(z - s, Z)).start()
                if 0 < s < 4:
                    dn_relay(k, wrap(z + s, Z)).start()

    def part_wait(s):
        lat_part(0, s, z).wait_recv()
        if 0 < s < 4:
            lat_part(1, s, z).wait_recv()

    def before(t):
        if t == 1:
            lat_step(3)
        elif t == 2:
            lat_spread(2)
            part_wait(1)
            prep_unit(jnp.int32(2))
        elif t == 3:
            part_wait(2)
        elif t == 4:
            lat_spread(3)
        elif t == 5:
            lat_spread(4)
            part_wait(3)
        elif t == 6:
            part_wait(4)

    def after(t):
        if t == 0:
            for k in (0, 1):
                st_near(k, 1).start()
        elif t == 1:
            dn_step(2)
            up_step(0, 2)
            up_x_all().wait_recv()
            up_start(1)
            up_start(2)
        elif t == 2:
            lat_step(4)
            for i in (0, 1):
                for k in (0, 1):
                    wo_near(k, i).start()
        elif t == 3:
            dn_step(3)
            up_step(0, 3)
        elif t == 4:
            up_step(1, 1)
            for k in (0, 1):
                st_near(k, 0).wait_recv()
                st_relay(k).start()
            dn_forward(0)
        elif t == 5:
            up_step(2, 1)
            dn_step(4)
            up_step(0, 4)
            for k in (0, 1):
                wo_near(k, 0).wait_recv()
                wo_relay(k).start()
        elif t == 6:
            up_step(1, 2)
        elif t == 7:
            up_step(2, 2)
            for k in (0, 1):
                wo_near(k, 1).wait_recv()
                wo_part(1 + 2 * k).start()

    def at(t, fn, times):
        for i in times:
            pl.when(t == i)(functools.partial(fn, i))

    def unit(t, carry):
        at(t, before, range(1, 7))
        va[...] = vna[...]
        vb[...] = vnb[...]
        @pl.when(t == 0)
        def _():
            first_unit()

        @pl.when(t == 1)
        def _():
            attend(range(X), lambda: None, lambda i: None)

        @pl.when((t > 1) & (t < 7))
        def _():
            attend(range(X), lambda: prep_unit(t + 1), lambda i: None)

        @pl.when(t == 7)
        def _():
            last_unit()

        at(t, after, range(8))
        return carry

    part_wait(0)
    prep_unit(jnp.int32(0))
    lax.fori_loop(0, 8, unit, 0)

    dn_part(0).start()
    up_step(1, 3)

    def merge(e):
        cols = slice(e * (TOK // 2), (e + 1) * (TOK // 2))
        for row, lo, width in ((0, 0, V_A), (2, V_A, V_B)):
            peaks = [srecv[i, row : row + 1, cols] for i in range(X)]
            top = functools.reduce(jnp.maximum, peaks)
            shares = [
                srecv[i, row + 1 : row + 2, cols] * jnp.exp2(peaks[i] - top) for i in range(X)
            ]
            inverse = 1.0 / (shares[0] + shares[1] + shares[2] + shares[3])
            mixed = orecv[0, lo : lo + width, cols].astype(F32) * (shares[0] * inverse)
            for i in range(1, X):
                mixed = mixed + orecv[i, lo : lo + width, cols].astype(F32) * (
                    shares[i] * inverse
                )
            att[y, pl.ds(lo, width), cols] = mixed.astype(BF16)
        for d in (2, 1, 3):
            a_y(d, e).start()

    def project(e):
        rows = slice(e * (TOK // 2), (e + 1) * (TOK // 2))
        attended = att[:, :, rows].reshape(Y * OUT, TOK // 2).T
        squares = jnp.zeros((TOK // 2, 1), F32)
        for n in range(4):
            cols = slice(n * 512, n * 512 + 512)
            mixed = mm(attended, wo[:, :, cols].reshape(Y * OUT, 512), NN)
            own = st[2 * e : 2 * e + 2, :, cols].reshape(TOK // 2, 512)
            summed = (own.astype(F32) + mixed).astype(BF16)
            res[rows, cols] = summed
            wide = summed.astype(F32)
            squares = squares + jnp.sum(wide * wide, axis=-1, keepdims=True)
        r = lax.rsqrt(squares * (1.0 / D) + EPSILON)
        for n in range(4):
            cols = slice(n * 512, n * 512 + 512)
            nrm[rows, cols] = (res[rows, cols].astype(F32) * r * ngain[:, cols]).astype(BF16)

    s_all().wait_recv()
    o_wait(0)
    merge(0)
    up_step(2, 3)
    o_wait(1)
    merge(1)
    wo_relay_all().wait_recv()
    wo_part(2).start()
    dn_forward(1)
    for d in (1, 3):
        dn_part(d).start()
    up_step(1, 4)
    for k in (0, 1):
        st_near(k, 1).wait_recv()
    st_relay_all().wait_recv()
    wo_part_all().wait_recv()
    a_wait(0)
    project(0)
    up_step(2, 4)
    dn_relay_all().wait_recv()
    dn_part(2).start()
    a_wait(1)
    project(1)
    up_part_all().wait_recv()
    for n in range(4):
        cols = slice(n * 256, n * 256 + 256)
        hidden = jnp.maximum(mm(nrm[...], up[:, :, :, :, cols].reshape(D, 256), NN), 0.0)
        act[:, cols] = (hidden * hidden).astype(BF16)

    dn_part_all().wait_recv()

    for n in range(4):
        weights = dn[2 * n : 2 * n + 2].reshape(512, FF)
        part = mm(act[...], weights, NT).astype(BF16)
        pb[n] = part.reshape(Y, OWN, 512)
        for k in (0, 1):
            r_half(k, n).start()

    for n in range(4):
        for k in (0, 1):
            r_half(k, n).wait_recv()
            dest = wrap(y + 1 - 2 * k, Y)
            cols = slice(k * 256, k * 256 + 256)
            pb[n, dest, :, cols] = (
                pb[n, dest, :, cols].astype(F32) + rh[k, n].astype(F32)
            ).astype(BF16)
            r_full(k, n).start()
    stores = [
        pltpu.make_async_copy(ob.at[n], out.at[:, pl.ds(n * 512, 512)], loc.at[n])
        for n in range(4)
    ]
    for n in range(4):
        cols = slice(n * 512, n * 512 + 512)
        total = pb[n, y].astype(F32)
        r_full_wait(n)
        for k in (0, 1):
            total = total + rb[k, n].astype(F32)
        ob[n] = (res[mine, cols].astype(F32) + total).astype(BF16)
        if n:
            stores[n - 1].start()
    stores[3].start()

    same(lat.at[pl.ds(0, 7), c, pl.ds(0, OWN + ROPE)], lat_s.at[0], lat_r.at[0], partner).wait_send()
    same(
        lat.at[pl.ds(0, 7), c, pl.ds(0, 3 * OWN)], laty_s.at[0], laty_r.at[0], partner
    ).wait_send()
    same(lat.at[:, c], latp_s.at[0], latp_r.at[0], partner).wait_send()
    same(dn.at[pl.ds(0, 7), x, c], dnz_s.at[0], dnz_r.at[0], partner).wait_send()
    same(st.at[pl.ds(0, 2)], st_s.at[0], st_r.at[0], partner).wait_send()
    same(wo.at[pl.ds(0, 2), :, half], wo_s.at[0], wo_r.at[0], partner).wait_send()
    q_all().wait_send()
    up_x_all().wait_send()
    up_ring_all().wait_send()
    up_part_all().wait_send()
    same(dn.at[:, pl.ds(0, 2), c], dnx_s.at[0], dnx_r.at[0, 0], partner).wait_send()
    dn_relay_all().wait_send()
    dn_part_all().wait_send()
    st_relay_all().wait_send()
    wo_relay_all().wait_send()
    wo_part_all().wait_send()
    o_all().wait_send()
    s_all().wait_send()
    a_all().wait_send()
    for k in (0, 1):
        r_half_all(k).wait_send()
        r_full_all(k).wait_send()
    for cp in stores:
        cp.wait()


def body(
    stream,
    query_a,
    query_b,
    latent,
    rotary_key,
    latent_gain,
    key_gain_a,
    key_gain_b,
    w_key_a,
    w_value_a,
    w_key_b,
    w_value_b,
    w_out_a,
    w_out_b,
    norm_gain,
    w_up,
    w_down,
):
    hbm = pl.BlockSpec(memory_space=pltpu.HBM)
    dma = pltpu.SemaphoreType.DMA
    return pl.pallas_call(
        kernel,
        out_shape=jax.ShapeDtypeStruct((OWN, D), BF16),
        in_specs=[hbm] * 17,
        out_specs=hbm,
        scratch_shapes=[
            pltpu.VMEM((RANK, NOPE_B), BF16),
            pltpu.VMEM((RANK, V_B), BF16),
            pltpu.VMEM((1, RANK), F32),
            pltpu.VMEM((1, DEPTH_A), F32),
            pltpu.VMEM((1, DEPTH_B), F32),
            pltpu.VMEM((1, D), F32),
            pltpu.VMEM((KV, RANK), BF16),
            pltpu.VMEM((DEPTH_A + DEPTH_B, TOK), F32),
            pltpu.VMEM((Z * C, ROPE, TOK), F32),
            pltpu.VMEM((4 * TOK, TOK), F32),
            pltpu.VMEM((4 * TOK, TOK), F32),
            pltpu.VMEM((Z, C, TOK + ROPE, RANK), BF16),
            pltpu.VMEM((X, TOK, DEPTH_A + DEPTH_B), BF16),
            pltpu.VMEM((Z, X, C, 32, FF), BF16),
            pltpu.VMEM((Z, X, C, 32, FF), BF16),
            pltpu.VMEM((Y, OUT, D), BF16),
            pltpu.VMEM((Y, OWN, D), BF16),
            pltpu.VMEM((256, TOK), BF16),
            pltpu.VMEM((256, TOK), BF16),
            pltpu.VMEM((2 * TOK, 256), BF16),
            pltpu.VMEM((2 * TOK, 256), BF16),
            pltpu.VMEM((V_A, 2 * TOK), BF16),
            pltpu.VMEM((V_B, 2 * TOK), BF16),
            pltpu.VMEM((V_A, 2 * TOK), BF16),
            pltpu.VMEM((V_B, 2 * TOK), BF16),
            pltpu.VMEM((X, OUT, TOK), F32),
            pltpu.VMEM((X, 8, TOK), F32),
            pltpu.VMEM((X, OUT, TOK), BF16),
            pltpu.VMEM((X, OUT, TOK), BF16),
            pltpu.VMEM((X, 8, TOK), F32),
            pltpu.VMEM((Y, OUT, TOK), BF16),
            pltpu.VMEM((TOK, D), BF16),
            pltpu.VMEM((TOK, D), BF16),
            pltpu.VMEM((TOK, FF), BF16),
            pltpu.VMEM((4, Y, OWN, 512), BF16),
            pltpu.VMEM((2, 4, OWN, 512), BF16),
            pltpu.VMEM((2, 4, OWN, 256), BF16),
            pltpu.VMEM((4, OWN, 512), BF16),
            dma((17,)),
            dma((1,)),
            dma((7,)),
            dma((1,)),
            dma((7,)),
            dma((1,)),
            dma((8,)),
            dma((1,)),
            dma((3,)),
            dma((1,)),
            dma((1,)),
            dma((1,)),
            dma((3, 7)),
            dma((1,)),
            dma((1,)),
            dma((1,)),
            dma((7,)),
            dma((2,)),
            dma((2, 2)),
            dma((1,)),
            dma((1,)),
            dma((1,)),
            dma((2,)),
            dma((2, 2)),
            dma((1,)),
            dma((2,)),
            dma((2, 2)),
            dma((1,)),
            dma((1,)),
            dma((1,)),
            dma((1,)),
            dma((2,)),
            dma((1,)),
            dma((1,)),
            dma((1,)),
            dma((2,)),
            dma((2,)),
            dma((2, 4)),
            dma((2,)),
            dma((4,)),
        ],
        compiler_params=pltpu.CompilerParams(
            collective_id=0, has_side_effects=True, vmem_limit_bytes=60 * 1024 * 1024,
        ),
        name="layer",
    )(
        latent,
        rotary_key.T,
        query_a.T,
        query_b.T,
        w_up,
        w_down.T,
        w_out_a,
        w_out_b,
        stream,
        w_key_a.T,
        w_key_b,
        w_value_a.T,
        w_value_b,
        latent_gain.reshape(1, RANK),
        key_gain_a.reshape(1, DEPTH_A),
        key_gain_b.reshape(1, DEPTH_B),
        norm_gain.reshape(1, D),
    )


def solution(mesh):
    in_specs = (
        P(("sp", "tp"), None),
        P("sp", "tp"),
        P("sp", "tp"),
        P("sp", None),
        P("sp", None),
        P(),
        P(),
        P(),
        P(None, "tp"),
        P(None, "tp"),
        P(None, "tp"),
        P(None, "tp"),
        P("tp", None),
        P("tp", None),
        P(),
        P("sp", "tp"),
        P("tp", "sp"),
    )
    out_specs = P(("sp", "tp"), None)
    return jax.shard_map(body, mesh=mesh, in_specs=in_specs, out_specs=out_specs, check_vma=False)
```
